128 devices in a mesh: sp: 16 (over z, y), tp: 8 (over x, core).
Axes of the slice: x: 4, y: 4, z: 4, core: 2. Of those that a mesh axis runs over, the one named last changes fastest.
Arguments:
- inputs: bfloat16 [16384, 4, 2048], P('sp'), may hold values from -6 to 6
- norm_gain: float32 [2048], replicated, may hold values from 0.1 to 1.9
- pool_proj: bfloat16 [2048, 1024], P(None, 'tp'), may hold values from -0.125 to 0.125
- pool_gate_proj: bfloat16 [2048, 1024], P(None, 'tp'), may hold values from -0.125 to 0.125
- pool_mix: bfloat16 [8, 128, 128], P('tp'), may hold values from -0.5 to 0.5
- query_proj: bfloat16 [2048, 1024], P(None, 'tp'), may hold values from -0.125 to 0.125
- key_proj: bfloat16 [2048, 512], P(None, 'tp'), may hold values from -0.125 to 0.125
- value_proj: bfloat16 [2048, 512], P(None, 'tp'), may hold values from -0.125 to 0.125
- attn_gate_proj: bfloat16 [2048, 1024], P(None, 'tp'), may hold values from -0.125 to 0.125
- query_gain: float32 [64], replicated, may hold values from 0.1 to 1.9
- key_gain: float32 [64], replicated, may hold values from 0.1 to 1.9
- sink_logit: float32 [16], P('tp'), may hold values from -12 to 240
- out_pool: bfloat16 [1024, 2048], P('sp'), may hold values from -0.125 to 0.125
- out_attn: bfloat16 [1024, 2048], P('sp'), may hold values from -0.125 to 0.125
Outputs:
- mixed_out: bfloat16 [16384, 4, 2048], P(('sp', 'tp'))
- log_weight_sum: float32 [16384, 4, 16], P('sp', None, 'tp')
The draws below stay inside these ranges and needn't reach their ends.
All inputs are finite; a program needn't handle non-finite values.
Results may differ from the reference program's by a relative error of at most 0.015.
Values may be sent and summed in bfloat16 or wider, within the bound.
A program may use at most 192 MiB of HBM per device.

```python
import jax
import jax.numpy as jnp
from jax import lax

D = 2048
POOL_GROUPS = 8
GROUP_CH = 128
POOL_WIDTH = 1024
HEADS = 16
KV_HEADS = 8
HEAD_DIM = 64
GROUP_SIZE = 2
ATT_WIDTH = 1024
KV_WIDTH = 512
WINDOW = 128
SEQS = 4
SEQ_LEN = 16384


def draw_sink_logit(key, part):
    base = jnp.clip(2.0 * jax.random.normal(jax.random.fold_in(key, 1), (HEADS,), jnp.float32), -12.0, 12.0)
    return base


def shard_levels(stream_key, dims, shards, least, top_value):
    def one(dim, blocks):
        heights = jax.random.uniform(jax.random.fold_in(jax.random.fold_in(stream_key, 6), dim), (blocks,), jnp.float32, least / len(shards), top_value / len(shards))
        return jnp.repeat(jnp.exp(heights), dims[dim] // blocks).reshape((-1,) + (1,) * (len(dims) - dim - 1))

    factor_of = one(*shards[0])
    for cut in shards[1:]:
        factor_of = factor_of * one(*cut)
    return factor_of


def centred(stream_key, dims, width, reach, pieces=(), held_as=jnp.bfloat16):
    drawn = width * jax.random.normal(stream_key, dims, jnp.float32)
    if pieces:
        drawn = drawn * shard_levels(stream_key, dims, pieces, -0.22, 0.18)
    return jnp.clip(drawn, -reach, reach).astype(held_as)


def setup_inputs(seed: int = 0) -> dict:
    splits = jax.random.split(jax.random.key(seed), 15)
    inputs = centred(splits[0], (SEQ_LEN, SEQS, D), 1.0, 6.0, ((0, 16),))
    norm_gain = jnp.clip(1.0 + 0.18 * jax.random.normal(splits[1], (D,), jnp.float32), 0.1, 1.9)
    pool_proj = centred(splits[2], (D, POOL_WIDTH), D ** -0.5, 0.125, ((1, 8),))
    pool_gate_proj = centred(splits[3], (D, POOL_WIDTH), D ** -0.5, 0.125, ((1, 8),))
    pool_mix = centred(splits[4], (POOL_GROUPS, GROUP_CH, GROUP_CH), GROUP_CH ** -0.5, 0.5, ((0, 8),))
    query_proj = centred(splits[5], (D, ATT_WIDTH), D ** -0.5, 0.125, ((1, 8),))
    key_proj = centred(splits[6], (D, KV_WIDTH), D ** -0.5, 0.125, ((1, 8),))
    value_proj = centred(splits[7], (D, KV_WIDTH), D ** -0.5, 0.125, ((1, 8),))
    attn_gate_proj = centred(splits[8], (D, ATT_WIDTH), D ** -0.5, 0.125, ((1, 8),))
    query_gain = jnp.clip(1.0 + 0.18 * jax.random.normal(splits[9], (HEAD_DIM,), jnp.float32), 0.1, 1.9)
    key_gain = jnp.clip(1.0 + 0.18 * jax.random.normal(splits[10], (HEAD_DIM,), jnp.float32), 0.1, 1.9)
    sink_logit = draw_sink_logit(jax.random.fold_in(splits[14], 71), 0)
    out_pool = centred(splits[12], (POOL_WIDTH, D), (POOL_WIDTH + ATT_WIDTH) ** -0.5, 0.125, ((0, 16),))
    out_attn = centred(splits[13], (ATT_WIDTH, D), (POOL_WIDTH + ATT_WIDTH) ** -0.5, 0.125, ((0, 16),))
    return {"inputs": inputs, "norm_gain": norm_gain, "pool_proj": pool_proj, "pool_gate_proj": pool_gate_proj, "pool_mix": pool_mix, "query_proj": query_proj, "key_proj": key_proj, "value_proj": value_proj, "attn_gate_proj": attn_gate_proj, "query_gain": query_gain, "key_gain": key_gain, "sink_logit": sink_logit, "out_pool": out_pool, "out_attn": out_attn}


EPS = 1e-06
NEG = -1e+30

def stored(values):
    return lax.optimization_barrier(values.astype(jnp.bfloat16))

def reference(inputs, norm_gain, pool_proj, pool_gate_proj, pool_mix, query_proj, key_proj, value_proj, attn_gate_proj, query_gain, key_gain, sink_logit, out_pool, out_attn):
    seq_len = inputs.shape[0]
    flt = inputs.astype(jnp.float32)
    hidden = stored(flt * lax.rsqrt(lax.optimization_barrier(jnp.mean(flt * flt, axis=-1, keepdims=True)) + EPS) * norm_gain.astype(jnp.float32))

    def project(weight):
        return stored(jnp.dot(hidden, weight, preferred_element_type=jnp.float32))
    pool_in = project(pool_proj)
    pool_gate = project(pool_gate_proj)
    queries = project(query_proj)
    key_rows = project(key_proj)
    value_rows = project(value_proj)
    attn_gate = project(attn_gate_proj)
    pool_f = pool_in.astype(jnp.float32).reshape(seq_len, SEQS, POOL_GROUPS, GROUP_CH)
    prefix = jnp.concatenate([jnp.zeros((1, SEQS, POOL_GROUPS, GROUP_CH), jnp.float32), jnp.cumsum(pool_f, axis=0)], axis=0)
    positions = jnp.arange(seq_len, dtype=jnp.int32)
    means = []
    for group_id in range(POOL_GROUPS):
        half_width = 2 ** (group_id % 4)
        low_pos = jnp.clip(positions - half_width, 0, seq_len - 1)
        high_pos = jnp.clip(positions + half_width - 1, 0, seq_len - 1)
        window_sum = prefix[high_pos + 1, :, group_id] - prefix[low_pos, :, group_id]
        count_live = (high_pos - low_pos + 1).astype(jnp.float32)[:, None, None]
        means.append(window_sum / count_live)
    pooled = stored(jnp.stack(means, axis=2) - pool_f)
    pool_mixed = jnp.einsum('lsgc,gcd->lsgd', pooled.astype(jnp.float32), pool_mix.astype(jnp.float32))
    pool_mixed = pool_mixed.reshape(seq_len, SEQS, POOL_WIDTH)
    y_pool = stored(pool_mixed * jax.nn.silu(pool_gate.astype(jnp.float32)))

    def head_norm(values, heads, gain):
        flt_heads = values.astype(jnp.float32).reshape(seq_len, SEQS, heads, HEAD_DIM)
        return stored(flt_heads * lax.rsqrt(lax.optimization_barrier(jnp.mean(flt_heads * flt_heads, axis=-1, keepdims=True)) + EPS) * gain.astype(jnp.float32))
    normed_q = head_norm(queries, HEADS, query_gain).reshape(seq_len, SEQS, KV_HEADS, GROUP_SIZE, HEAD_DIM)
    normed_k = head_norm(key_rows, KV_HEADS, key_gain)
    value_heads = value_rows.reshape(seq_len, SEQS, KV_HEADS, HEAD_DIM)
    padding = ((WINDOW, WINDOW), (0, 0), (0, 0), (0, 0))
    key_pad = jnp.pad(normed_k, padding)
    value_pad = jnp.pad(value_heads, padding)
    slopes = (2.0 ** (-8.0 * jnp.arange(1, HEADS + 1, dtype=jnp.float32) / HEADS)).reshape(KV_HEADS, GROUP_SIZE)
    sink_vals = sink_logit.astype(jnp.float32).reshape(KV_HEADS, GROUP_SIZE)[None, :, :, None]

    def block(index):
        query_block = lax.dynamic_slice_in_dim(normed_q, index * WINDOW, WINDOW, 0)
        key_block = lax.dynamic_slice_in_dim(key_pad, index * WINDOW, 3 * WINDOW, 0)
        value_block = lax.dynamic_slice_in_dim(value_pad, index * WINDOW, 3 * WINDOW, 0)
        scores = jnp.einsum('qskgd,jskd->skgqj', query_block.astype(jnp.float32), key_block.astype(jnp.float32)) * HEAD_DIM ** (-0.5)
        query_pos = index * WINDOW + jnp.arange(WINDOW, dtype=jnp.int32)
        key_pos = index * WINDOW - WINDOW + jnp.arange(3 * WINDOW, dtype=jnp.int32)
        distance = jnp.abs(query_pos[:, None] - key_pos[None, :])
        usable = (distance <= WINDOW) & (key_pos >= 0)[None, :] & (key_pos < seq_len)[None, :]
        scores = scores - slopes[None, :, :, None, None] * distance.astype(jnp.float32)
        scores = jnp.where(usable, scores, NEG)
        row_top = jnp.maximum(lax.optimization_barrier(jnp.max(scores, axis=-1)), sink_vals)
        weights = jnp.exp(scores - row_top[..., None])
        weight_total = lax.optimization_barrier(jnp.sum(weights, axis=-1)) + jnp.exp(sink_vals - row_top)
        log_sum = row_top + jnp.log(weight_total)
        attended = jnp.einsum('skgqj,jskd->qskgd', stored(weights).astype(jnp.float32), value_block.astype(jnp.float32))
        attended = attended / jnp.transpose(weight_total, (3, 0, 1, 2))[..., None]
        return (attended.reshape(WINDOW, SEQS, ATT_WIDTH), jnp.transpose(log_sum, (3, 0, 1, 2)).reshape(WINDOW, SEQS, HEADS))
    attended, log_sums = lax.map(block, jnp.arange(seq_len // WINDOW, dtype=jnp.int32))
    attended = attended.reshape(seq_len, SEQS, ATT_WIDTH)
    log_weight_sum = log_sums.reshape(seq_len, SEQS, HEADS)
    y_attn = stored(attended * jax.nn.silu(attn_gate.astype(jnp.float32)))
    summed = jnp.dot(y_pool, out_pool, preferred_element_type=jnp.float32) + jnp.dot(y_attn, out_attn, preferred_element_type=jnp.float32)
    return (summed.astype(jnp.bfloat16), log_weight_sum)
```

```python
import functools

import jax
import jax.numpy as jnp
from jax import lax
from jax.experimental import pallas as pl
from jax.experimental.pallas import tpu as pltpu
from jax.sharding import PartitionSpec as P

HEADS = 16
EPS = 1e-06
NEG = -1e30
SHIFT = 29.5
LOG2E = 1.4426950408889634
BF = jnp.bfloat16
F32 = jnp.float32
SEQ_LEN = 16384
NSP = 16
COMM = True


def split_dot(values, ones):
    hi = values.astype(BF)
    lo = (values - hi.astype(F32)).astype(BF)
    return jnp.dot(hi, ones, preferred_element_type=F32) + jnp.dot(lo, ones, preferred_element_type=F32)


def silu(v):
    return v / (1.0 + jnp.exp(-v))


def kernel(
    x_hbm, gain, pw, gw, qw, kw, vw, aw, mix, qg, kg, sink, outp, outa,
    out, lse,
    xb, wb, kst, vst, tmp, qs, kvs, poolbuf, gate, agate, bias, band, ysend, yr, wg, acc, att, lseb,
    xsem, wsem, asend, arecv, hsend, hrecv, gsend, grecv, dsend, drecv,
):
    if COMM:
        sp = lax.axis_index("sp")
        tp = lax.axis_index("tp")
    else:
        sp = jnp.int32(0)
        tp = jnp.int32(0)
    chip = tp // 2
    c = tp % 2
    y = sp % 4
    z = sp // 4
    a = y * (1 - c) + z * c
    b_ = z * (1 - c) + y * c
    sa = 1 + 3 * c
    sb = 4 - 3 * c

    def order(k):
        return (2 * chip + 1 - c + k - 2 * c * k + 16) % 8

    def xcopy(k):
        return pltpu.make_async_copy(
            x_hbm.at[pl.ds(order(k) * 128, 128)], xb.at[k % 2], xsem.at[k % 2]
        )

    wcopies = [
        pltpu.make_async_copy(outp, wg.at[0, sp], wsem.at[0]),
        pltpu.make_async_copy(outa, wg.at[1, sp], wsem.at[1]),
        pltpu.make_async_copy(pw, wb.at[:, pl.ds(0, 128)], wsem.at[2]),
        pltpu.make_async_copy(gw, wb.at[:, pl.ds(128, 128)], wsem.at[3]),
        pltpu.make_async_copy(qw, wb.at[:, pl.ds(256, 128)], wsem.at[4]),
        pltpu.make_async_copy(kw, kst, wsem.at[5]),
        pltpu.make_async_copy(vw, vst, wsem.at[6]),
        pltpu.make_async_copy(aw, wb.at[:, pl.ds(512, 128)], wsem.at[7]),
    ]
    for cp in wcopies:
        cp.start()
    xcopy(0).start()
    xcopy(1).start()

    zeros = jnp.zeros((64, 128), BF)
    poolbuf[0:64, :] = zeros
    poolbuf[64 + 4096 : 128 + 4096, :] = zeros
    for s in range(4):
        kvs[s, 0:128, :] = jnp.zeros((128, 128), BF)
        kvs[s, 9 * 128 : 10 * 128, :] = jnp.zeros((128, 128), BF)

    def remote(src, dst, ss, rs, dev):
        return pltpu.make_async_remote_copy(
            src_ref=src, dst_ref=dst, send_sem=ss, recv_sem=rs,
            device_id=dev, device_id_type=pl.DeviceIdType.MESH,
        )

    if COMM:
        barrier = pltpu.get_barrier_semaphore()

        def greet(dev):
            pl.semaphore_signal(barrier, inc=1, device_id=dev, device_id_type=pl.DeviceIdType.MESH)

        for j in range(1, 8):
            greet((sp, (tp + j) % 8))
        greet((z * 4 + (y + 1) % 4, tp))
        greet((z * 4 + (y + 3) % 4, tp))
        greet((((z + 1) % 4) * 4 + y, tp))
        greet((((z + 3) % 4) * 4 + y, tp))

        greet(((sp + 1) % NSP, tp))
        greet(((sp + NSP - 1) % NSP, tp))
        pl.semaphore_wait(barrier, 13)

    def slice_at(da, db):
        return ((a + da) % 4) * sa + ((b_ + db) % 4) * sb

    def piece(da, db, half):
        if half is None:
            return wg.at[c, slice_at(da, db)]
        return wg.at[c, slice_at(da, db), pl.ds(32 * half, 32)]

    sends = []

    def gcopy(da, db, half, ma, mb, n):
        return remote(
            piece(da, db, half), piece(da, db, half), gsend.at[n],
            grecv.at[((da - ma) % 4) * 4 + (db - mb) % 4, half or 0],
            (slice_at(ma, mb), tp),
        )

    def send(da, db, half, ma, mb):
        if COMM:
            n = len(sends)
            sends.append((da, db, half, ma, mb, n))
            gcopy(da, db, half, ma, mb, n).start()

    def got(da, db, half=None):
        if COMM:
            ref = piece(da, db, half)
            remote(
                ref, ref, gsend.at[0], grecv.at[da * 4 + db, half or 0], (sp, tp + 1 - 2 * c)
            ).wait_recv()

    def across(da, db):
        ref = piece(da, db, None)
        return remote(
            ref, ref, dsend.at[da * 4 + db], drecv.at[da * 4 + db], (sp, tp + 1 - 2 * c)
        )

    def share(da, db):
        if COMM:
            across(da, db).start()

    def event0():
        send(0, 0, None, 1, 0)
        send(0, 0, None, -1, 0)
        send(0, 0, None, 0, 1)
        send(0, 0, None, 0, -1)

    def event1():
        got(3, 0)
        send(3, 0, 0, 1, 0)
        got(1, 0)
        send(1, 0, 1, -1, 0)
        for da in (3, 1):
            send(da, 0, None, 0, 1)
            send(da, 0, None, 0, -1)
            share(da, 0)

    def through(da):
        got(da, 3)
        send(da, 3, 0, 0, 1)
        share(da, 3)
        got(da, 1)
        send(da, 1, 1, 0, -1)
        share(da, 1)

    def far(da):
        got(da, 2, 0)
        got(da, 2, 1)
        share(da, 2)

    def event2():
        got(2, 0, 0)
        got(2, 0, 1)
        send(2, 0, None, 0, 1)
        send(2, 0, None, 0, -1)
        share(2, 0)
        through(0)

    def event3():
        through(3)
        through(1)
        far(0)

    def event4():
        through(2)
        far(3)
        far(1)

    def event5():
        far(2)

    wcopies[0].wait()
    wcopies[1].wait()
    event0()

    lane = lax.broadcasted_iota(jnp.int32, (1, 128), 1)
    low = lane < 64
    ones = jnp.ones((128, 128), BF)
    head_ones = (
        (lax.broadcasted_iota(jnp.int32, (128, 128), 0) // 64)
        == (lax.broadcasted_iota(jnp.int32, (128, 128), 1) // 64)
    ).astype(F32).astype(BF)

    tpf = tp.astype(F32)
    s0 = sink[0]
    s1 = sink[1]
    m0 = jnp.maximum(s0, SHIFT)
    m1 = jnp.maximum(s1, SHIFT)
    for h in range(2):
        slope = jnp.exp2(jnp.full((128, 128), -(2.0 * tpf + (h + 1.0)) * 0.5, F32))
        m = (m0, m1)[h]
        for p in range(3):
            i = lax.broadcasted_iota(jnp.int32, (128, 128), 0)
            j = lax.broadcasted_iota(jnp.int32, (128, 128), 1)
            dist = jnp.abs(i - j - (128 * p - 128))
            val = (-slope * dist.astype(F32) - m) * LOG2E
            bias[p, 128 * h : 128 * h + 128, :] = jnp.where(dist <= 128, val, NEG)
        bias[3, 128 * h : 128 * h + 128, :] = jnp.full((128, 128), NEG, F32)

    hw = jnp.left_shift(jnp.int32(1), tp % 4)
    delta = (
        lax.broadcasted_iota(jnp.int32, (128, 256), 1)
        - 64
        - lax.broadcasted_iota(jnp.int32, (128, 256), 0)
    )
    band[...] = (
        ((delta + 1024) % 4 == 0) & (delta >= -4 * hw) & (delta <= 4 * hw - 4)
    ).astype(F32).astype(BF)

    for cp in wcopies[2:]:
        cp.wait()

    def prep(l, carry):
        rows = pl.ds(pl.multiple_of(l * 128, 128), 128)
        g = jnp.transpose(jnp.broadcast_to(gain[pl.ds(l, 1), :], (128, 128)))
        for t in (0, 1, 2, 4):
            cols = slice(128 * t, 128 * t + 128)
            wb[rows, cols] = (wb[rows, cols].astype(F32) * g).astype(BF)
        kv = jnp.concatenate([kst[rows, :].astype(F32), vst[rows, :].astype(F32)], axis=1)
        wb[rows, 384:512] = (kv * g).astype(BF)
        return carry

    lax.fori_loop(0, 16, prep, 0)

    qgain = jnp.concatenate([qg[...], qg[...]], axis=1) * (0.125 * LOG2E)
    kgain = jnp.concatenate([kg[...], kg[...]], axis=1)

    def halo(i, src, dst, dev):
        return remote(src, dst, hsend.at[i], hrecv.at[i], dev)

    def halo_left():
        return (
            halo(0, kvs.at[:, pl.ds(128, 128), :], kvs.at[:, pl.ds(9 * 128, 128), :], (sp - 1, tp)),
            halo(1, poolbuf.at[pl.ds(64, 32)], poolbuf.at[pl.ds(64 + 4096, 32)], (sp - 1, tp)),
        )

    def halo_right():
        return (
            halo(2, kvs.at[:, pl.ds(8 * 128, 128), :], kvs.at[:, pl.ds(0, 128), :], (sp + 1, tp)),
            halo(3, poolbuf.at[pl.ds(64 + 4096 - 32, 32)], poolbuf.at[pl.ds(32, 32)], (sp + 1, tp)),
        )

    def project(k, blk):
        xcopy(k).wait()
        x = xb[k % 2].reshape(512, 2048)
        sq = jnp.zeros((512, 128), F32)
        for l in range(16):
            t = x[:, 128 * l : 128 * l + 128].astype(F32)
            sq = sq + t * t
        r = lax.rsqrt(split_dot(sq, ones) * (1.0 / 2048) + EPS)
        p = jnp.dot(x, wb[...], preferred_element_type=F32)
        rows = pl.ds(pl.multiple_of(blk * 512, 512), 512)
        prows = pl.ds(pl.multiple_of(blk * 512 + 64, 64), 512)
        poolbuf[prows, :] = (p[:, 0:128] * r).astype(BF)
        gate[rows, :] = (p[:, 128:256] * r).astype(BF)
        agate[rows, :] = (p[:, 512:640] * r).astype(BF)
        q = (p[:, 256:384] * r).astype(BF).astype(F32)
        rq = lax.rsqrt(split_dot(q * q, head_ones) * (1.0 / 64) + EPS)
        tmp[0] = q * rq * qgain
        kv = (p[:, 384:512] * r).astype(BF).astype(F32)
        rk = lax.rsqrt(split_dot(kv * kv, head_ones) * (1.0 / 64) + EPS)
        tmp[1] = jnp.where(low, kv * rk * kgain, kv)
        for s in range(4):
            q = tmp[0, pl.ds(s, 128, stride=4), :]
            qs[blk, s, 0:128, :] = jnp.where(low, q, 0.0).astype(BF)
            qs[blk, s, 128:256, :] = jnp.where(low, pltpu.roll(q, 64, 1), 0.0).astype(BF)
            kvs[s, pl.ds(pl.multiple_of((blk + 1) * 128, 128), 128), :] = tmp[
                1, pl.ds(s, 128, stride=4), :
            ].astype(BF)

        @pl.when(k + 2 < 8)
        def _():
            xcopy(k + 2).start()

        if COMM:
            @pl.when((blk == 0) & (sp > 0))
            def _():
                for cp in halo_left():
                    cp.start()

            @pl.when((blk == 7) & (sp < NSP - 1))
            def _():
                for cp in halo_right():
                    cp.start()

    def emit(part, blk, value):
        @pl.when(blk == tp)
        def _():
            yr[part, blk] = value

        @pl.when(blk != tp)
        def _():
            ysend[part, blk] = value
            if COMM:
                remote(
                    ysend.at[part, blk], yr.at[part, tp], asend.at[part, blk], arecv.at[part, tp], (sp, blk)
                ).start()

    def pool(blk):
        if COMM:
            @pl.when((blk == 0) & (sp > 0))
            def _():
                halo_right()[1].wait_recv()

            @pl.when((blk == 7) & (sp < NSP - 1))
            def _():
                halo_left()[1].wait_recv()

        start = pl.multiple_of(blk * 512, 512)
        sums = jnp.concatenate(
            [
                jnp.dot(band[...], poolbuf[pl.ds(start + 128 * g, 256), :], preferred_element_type=F32)
                for g in range(4)
            ],
            axis=0,
        )
        pos = sp * 1024 + blk * 128 + lax.broadcasted_iota(jnp.int32, (512, 128), 0) // 4
        lo = jnp.maximum(pos - hw, 0)
        hi = jnp.minimum(pos + hw - 1, SEQ_LEN - 1)
        count = (hi - lo + 1).astype(F32)
        own = poolbuf[pl.ds(start + 64, 512), :].astype(F32)
        pooled = (sums / count - own).astype(BF)
        mixed = jnp.dot(pooled, mix[0], preferred_element_type=F32)
        g = gate[pl.ds(start, 512), :].astype(F32)
        emit(0, blk, (mixed * silu(g)).astype(BF))

    def proj_step(k, carry):
        project(k, order(k))

        @pl.when(k >= 3)
        def _():
            pool(order(k - 2))

        if COMM:
            for at, event in ((2, event1), (4, event2), (6, event3)):
                pl.when(k == at)(event)
        return carry

    lax.fori_loop(0, 8, proj_step, 0)

    def pool_rest(k, carry):
        pool(order(k % 8))
        return carry

    lax.fori_loop(6, 9, pool_rest, 0)

    sp0 = 1 - (sp + 15) // 16
    sp15 = (sp + 1) // 16

    def attend(blk):
        if COMM:
            @pl.when((blk == 0) & (sp > 0))
            def _():
                halo_right()[0].wait_recv()

            @pl.when((blk == 7) & (sp < NSP - 1))
            def _():
                halo_left()[0].wait_recv()

        left = 3 * sp0 * (1 - (blk + 7) // 8)
        right = 2 + sp15 * ((blk + 1) // 8)
        for s in range(4):
            q = qs[blk, s]
            kv = kvs[s, pl.ds(pl.multiple_of(blk * 128, 128), 384), :]
            scores = lax.dot_general(q, kv, (((1,), (1,)), ((), ())), preferred_element_type=F32)
            w = jnp.concatenate(
                [
                    jnp.exp2(scores[:, 128 * p : 128 * p + 128] + bias[at]).astype(BF)
                    for p, at in ((0, left), (1, 1), (2, right))
                ],
                axis=1,
            )
            rhs = jnp.concatenate([kv, jnp.ones((384, 128), BF)], axis=1)
            o = jnp.dot(w, rhs, preferred_element_type=F32)
            t0 = o[0:128, 128:256] + jnp.exp(jnp.full((128, 128), s0 - m0, F32))
            t1 = o[128:256, 128:256] + jnp.exp(jnp.full((128, 128), s1 - m1, F32))
            both = jnp.where(
                low, pltpu.roll(o[0:128, 0:128], 64, 1) / t0, o[128:256, 0:128] / t1
            )
            att[pl.ds(s, 128, stride=4), :] = both
            lseb[pl.ds(s, 128, stride=4), :] = jnp.where(
                lane == 0, m0 + jnp.log(t0), m1 + jnp.log(t1)
            )
        g = agate[pl.ds(pl.multiple_of(blk * 512, 512), 512), :].astype(F32)
        emit(1, blk, (att[...] * silu(g)).astype(BF))
        lse[pl.ds(pl.multiple_of(blk * 128, 128), 128)] = lseb[:, 0:2].reshape(128, 4, 2)

    def att_step(k, carry):
        j = k // 2
        d = (2 + 3 * j + 3 * (j // 2) + 2 * (j // 3)) % 4
        d = (d + c * (4 - 2 * d)) % 4
        attend(((chip + d) % 4) * 2 + (c + 1 + k) % 2)
        if COMM:
            for at, event in ((1, event4), (5, event5)):
                pl.when(k == at)(event)
        return carry

    lax.fori_loop(0, 8, att_step, 0)

    def exchange(part, j):
        return remote(
            ysend.at[part, j], yr.at[part, tp], asend.at[part, j], arecv.at[part, j], (sp, j)
        )

    def arrive(part):
        if COMM:
            for j in range(8):
                @pl.when(tp != j)
                def _():
                    remote(
                        ysend.at[part, j], yr.at[part, j], asend.at[part, j], arecv.at[part, j], (sp, j)
                    ).wait_recv()

    if COMM:
        for da in range(4):
            for db in range(4):
                if da or db:
                    ref = wg.at[1 - c, ((b_ + da) % 4) * sb + ((a + db) % 4) * sa]
                    remote(
                        ref, ref, dsend.at[da * 4 + db], drecv.at[da * 4 + db], (sp, tp + 1 - 2 * c)
                    ).wait_recv()

    arrive(0)

    def out_pool_step(n, carry):
        cols = pl.ds(pl.multiple_of(n * 256, 256), 256)
        acts = jnp.concatenate([yr[0, j] for j in range(8)], axis=1)
        acc[:, cols] = jnp.dot(
            acts, wg[0, :, :, cols].reshape(1024, 256), preferred_element_type=F32
        )
        return carry

    lax.fori_loop(0, 8, out_pool_step, 0)
    arrive(1)

    def out_attn_step(n, carry):
        cols = pl.ds(pl.multiple_of(n * 256, 256), 256)
        acts = jnp.concatenate([yr[1, j] for j in range(8)], axis=1)
        total = acc[:, cols] + jnp.dot(
            acts, wg[1, :, :, cols].reshape(1024, 256), preferred_element_type=F32
        )
        out[:, :, cols] = total.astype(BF).reshape(128, 4, 256)
        return carry

    lax.fori_loop(0, 8, out_attn_step, 0)

    if COMM:
        for part in range(2):
            for j in range(8):
                @pl.when(tp != j)
                def _():
                    exchange(part, j).wait_send()
        for item in sends:
            gcopy(*item).wait_send()
        for da in range(4):
            for db in range(4):
                if da or db:
                    across(da, db).wait_send()

        @pl.when(sp > 0)
        def _():
            for cp in halo_left():
                cp.wait_send()

        @pl.when(sp < NSP - 1)
        def _():
            for cp in halo_right():
                cp.wait_send()


def layer(
    inputs, norm_gain, pool_proj, pool_gate_proj, pool_mix, query_proj, key_proj, value_proj,
    attn_gate_proj, query_gain, key_gain, sink_logit, out_pool, out_attn,
):
    hbm = pl.BlockSpec(memory_space=pl.ANY)
    vmem = pl.BlockSpec(memory_space=pltpu.VMEM)
    smem = pl.BlockSpec(memory_space=pltpu.SMEM)
    dma = pltpu.SemaphoreType.DMA
    return pl.pallas_call(
        kernel,
        out_shape=(
            jax.ShapeDtypeStruct((128, 4, 2048), BF),
            jax.ShapeDtypeStruct((1024, 4, 2), F32),
        ),
        in_specs=[hbm, vmem, hbm, hbm, hbm, hbm, hbm, hbm, vmem, vmem, vmem, smem, hbm, hbm],
        out_specs=(vmem, vmem),
        scratch_shapes=[
            pltpu.VMEM((2, 128, 4, 2048), BF),
            pltpu.VMEM((2048, 640), BF),
            pltpu.VMEM((2048, 64), BF),
            pltpu.VMEM((2048, 64), BF),
            pltpu.VMEM((2, 512, 128), F32),
            pltpu.VMEM((8, 4, 256, 128), BF),
            pltpu.VMEM((4, 1280, 128), BF),
            pltpu.VMEM((4096 + 128, 128), BF),
            pltpu.VMEM((4096, 128), BF),
            pltpu.VMEM((4096, 128), BF),
            pltpu.VMEM((4, 256, 128), F32),
            pltpu.VMEM((128, 256), BF),
            pltpu.VMEM((2, 8, 512, 128), BF),
            pltpu.VMEM((2, 8, 512, 128), BF),
            pltpu.VMEM((2, 16, 64, 2048), BF),
            pltpu.VMEM((512, 2048), F32),
            pltpu.VMEM((512, 128), F32),
            pltpu.VMEM((512, 128), F32),
            dma((2,)), dma((8,)),
            dma((2, 8)), dma((2, 8)),
            dma((4,)), dma((4,)),
            dma((24,)), dma((16, 2)),
            dma((16,)), dma((16,)),
        ],
        compiler_params=pltpu.CompilerParams(
            vmem_limit_bytes=60 * 1024 * 1024,
            **(dict(collective_id=0, has_side_effects=True) if COMM else {}),
        ),
        name="mixer_layer",
    )(
        inputs, norm_gain.reshape(16, 128), pool_proj, pool_gate_proj, query_proj, key_proj,
        value_proj, attn_gate_proj, pool_mix, query_gain.reshape(1, 64), key_gain.reshape(1, 64),
        sink_logit, out_pool, out_attn,
    )


def solution(mesh):
    placed = (
        P("sp", None, None), P(), P(None, "tp"), P(None, "tp"), P("tp", None, None), P(None, "tp"),
        P(None, "tp"), P(None, "tp"), P(None, "tp"), P(), P(), P("tp"), P("sp", None), P("sp", None),
    )
    return jax.shard_map(
        layer,
        mesh=mesh,
        in_specs=placed,
        out_specs=(P(("sp", "tp"), None, None), P("sp", None, "tp")),
        check_vma=False,
    )
```

```python
import functools

import jax
import jax.numpy as jnp
from jax import lax
from jax.experimental import pallas as pl
from jax.experimental.pallas import tpu as pltpu
from jax.sharding import PartitionSpec as P

HEADS = 16
EPS = 1e-06
NEG = -1e30
SHIFT = 29.5
LOG2E = 1.4426950408889634
BF = jnp.bfloat16
F32 = jnp.float32
SEQ_LEN = 16384
NSP = 16
COMM = True


def split_dot(values, ones):
    hi = values.astype(BF)
    lo = (values - hi.astype(F32)).astype(BF)
    return jnp.dot(hi, ones, preferred_element_type=F32) + jnp.dot(lo, ones, preferred_element_type=F32)


def silu(v):
    return v / (1.0 + jnp.exp(-v))


def kernel(
    x_hbm, gain, pw, gw, qw, kw, vw, aw, mix, qg, kg, sink, outp, outa,
    out, lse,
    xa, xc, xo, wb, kvt, pa, pc, tmp, inv, rsend, rbuf, qs, kvs, poolbuf, gate, agate, bias, band, ysend, yr, wg, acc, att,
    xsem, wsem, rs_send, rs_recv, asend, arecv, hsend, hrecv, gsend, grecv, dsend, drecv,
):
    if COMM:
        sp = lax.axis_index("sp")
        tp = lax.axis_index("tp")
    else:
        sp = jnp.int32(0)
        tp = jnp.int32(0)
    chip = tp // 2
    c = tp % 2
    y = sp % 4
    z = sp // 4
    a = y * (1 - c) + z * c
    b_ = z * (1 - c) + y * c
    sa = 1 + 3 * c
    sb = 4 - 3 * c

    def order(k):
        return (2 * chip + 1 - c + k - 2 * c * k + 16) % 8

    def xcopy(k):
        return pltpu.make_async_copy(
            x_hbm.at[pl.ds(order(k) * 128, 128)], (xa, xc)[k % 2], xsem.at[k % 2]
        )

    xown = pltpu.make_async_copy(x_hbm.at[pl.ds(tp * 128, 128)], xo, xsem.at[2])
    xown.start()

    wcopies = [
        pltpu.make_async_copy(outp, wg.at[0, sp], wsem.at[0]),
        pltpu.make_async_copy(outa, wg.at[1, sp], wsem.at[1]),
        pltpu.make_async_copy(pw, wb.at[:, pl.ds(0, 128)], wsem.at[2]),
        pltpu.make_async_copy(gw, wb.at[:, pl.ds(128, 128)], wsem.at[3]),
        pltpu.make_async_copy(qw, wb.at[:, pl.ds(256, 128)], wsem.at[4]),
        pltpu.make_async_copy(kw, kvt.at[pl.ds(0, 64)], wsem.at[5]),
        pltpu.make_async_copy(vw, kvt.at[pl.ds(64, 64)], wsem.at[6]),
        pltpu.make_async_copy(aw, wb.at[:, pl.ds(512, 128)], wsem.at[7]),
    ]
    for cp in wcopies:
        cp.start()
    xcopy(0).start()
    xcopy(1).start()

    zeros = jnp.zeros((64, 128), BF)
    poolbuf[0:64, :] = zeros
    poolbuf[64 + 4096 : 128 + 4096, :] = zeros
    for s in range(4):
        kvs[s, 0:128, :] = jnp.zeros((128, 128), BF)
        kvs[s, 9 * 128 : 10 * 128, :] = jnp.zeros((128, 128), BF)

    def remote(src, dst, ss, rs, dev):
        return pltpu.make_async_remote_copy(
            src_ref=src, dst_ref=dst, send_sem=ss, recv_sem=rs,
            device_id=dev, device_id_type=pl.DeviceIdType.MESH,
        )

    if COMM:
        barrier = pltpu.get_barrier_semaphore()

        def greet(dev):
            pl.semaphore_signal(barrier, inc=1, device_id=dev, device_id_type=pl.DeviceIdType.MESH)

        for j in range(1, 8):
            greet((sp, (tp + j) % 8))
        greet((z * 4 + (y + 1) % 4, tp))
        greet((z * 4 + (y + 3) % 4, tp))
        greet((((z + 1) % 4) * 4 + y, tp))
        greet((((z + 3) % 4) * 4 + y, tp))

        greet(((sp + 1) % NSP, tp))
        greet(((sp + NSP - 1) % NSP, tp))

    sp0 = 1 - (sp + 15) // 16
    sp15 = (sp + 1) // 16

    def slice_at(da, db):
        return ((a + da) % 4) * sa + ((b_ + db) % 4) * sb

    def piece(da, db, half):
        if half is None:
            return wg.at[c, slice_at(da, db)]
        return wg.at[c, slice_at(da, db), pl.ds(32 * half, 32)]

    sends = []

    def gcopy(da, db, half, ma, mb, n):
        return remote(
            piece(da, db, half), piece(da, db, half), gsend.at[n],
            grecv.at[((da - ma) % 4) * 4 + (db - mb) % 4, half or 0],
            (slice_at(ma, mb), tp),
        )

    def send(da, db, half, ma, mb):
        if COMM:
            n = len(sends)
            sends.append((da, db, half, ma, mb, n))
            gcopy(da, db, half, ma, mb, n).start()

    def got(da, db, half=None):
        if COMM:
            ref = piece(da, db, half)
            remote(
                ref, ref, gsend.at[0], grecv.at[da * 4 + db, half or 0], (sp, tp + 1 - 2 * c)
            ).wait_recv()

    def across(da, db):
        ref = piece(da, db, None)
        return remote(
            ref, ref, dsend.at[da * 4 + db], drecv.at[da * 4 + db], (sp, tp + 1 - 2 * c)
        )

    def share(da, db):
        if COMM:
            across(da, db).start()

    def event0():
        send(0, 0, None, 1, 0)
        send(0, 0, None, -1, 0)
        send(0, 0, None, 0, 1)
        send(0, 0, None, 0, -1)

    def event1():
        got(3, 0)
        send(3, 0, 0, 1, 0)
        got(1, 0)
        send(1, 0, 1, -1, 0)
        for da in (3, 1):
            send(da, 0, None, 0, 1)
            send(da, 0, None, 0, -1)
            share(da, 0)

    def through(da):
        got(da, 3)
        send(da, 3, 0, 0, 1)
        share(da, 3)
        got(da, 1)
        send(da, 1, 1, 0, -1)
        share(da, 1)

    def far(da):
        got(da, 2, 0)
        got(da, 2, 1)
        share(da, 2)

    def event2():
        got(2, 0, 0)
        got(2, 0, 1)
        send(2, 0, None, 0, 1)
        send(2, 0, None, 0, -1)
        share(2, 0)
        through(0)

    def event3():
        through(3)
        through(1)
        far(0)

    def event4():
        through(2)
        far(3)
        far(1)

    def event5():
        far(2)

    lane = lax.broadcasted_iota(jnp.int32, (1, 128), 1)
    low = lane < 64
    ones = jnp.ones((128, 128), BF)
    row128 = lax.broadcasted_iota(jnp.int32, (128, 128), 0)
    col128 = lax.broadcasted_iota(jnp.int32, (128, 128), 1)
    head_ones = ((row128 // 64) == (col128 // 64)).astype(F32).astype(BF)

    xown.wait()
    x = xo[...].reshape(512, 2048)
    sq = jnp.zeros((512, 128), F32)
    for l in range(16):
        t = x[:, 128 * l : 128 * l + 128].astype(F32)
        sq = sq + t * t
    r = lax.rsqrt(split_dot(sq, ones) * (1.0 / 2048) + EPS)
    packed = [
        jnp.sum(jnp.where(row128 == col128, r[128 * g : 128 * g + 128], 0.0), axis=0, keepdims=True)
        for g in range(4)
    ]
    packed = jnp.concatenate(packed + [jnp.zeros((4, 128), F32)], axis=0)
    rsend[...] = packed
    rbuf[tp] = packed

    def rcopy(j, at):
        return remote(rsend, rbuf.at[at], rs_send.at[j], rs_recv.at[at], (sp, j))

    if COMM:
        pl.semaphore_wait(barrier, 13)

    if COMM:
        for j in range(8):
            @pl.when(tp != j)
            def _():
                rcopy(j, tp).start()

    wcopies[0].wait()
    wcopies[1].wait()
    event0()

    tpf = tp.astype(F32)
    s0 = sink[0]
    s1 = sink[1]
    m0 = jnp.maximum(s0, SHIFT)
    m1 = jnp.maximum(s1, SHIFT)
    for h in range(2):
        slope = jnp.exp2(jnp.full((128, 128), -(2.0 * tpf + (h + 1.0)) * 0.5, F32))
        m = (m0, m1)[h]
        for p in range(3):
            i = lax.broadcasted_iota(jnp.int32, (128, 128), 0)
            j = lax.broadcasted_iota(jnp.int32, (128, 128), 1)
            dist = jnp.abs(i - j - (128 * p - 128))
            val = (-slope * dist.astype(F32) - m) * LOG2E
            bias[p, 128 * h : 128 * h + 128, :] = jnp.where(dist <= 128, val, NEG)
        bias[3, 128 * h : 128 * h + 128, :] = jnp.full((128, 128), NEG, F32)

    hw = jnp.left_shift(jnp.int32(1), tp % 4)
    delta = (
        lax.broadcasted_iota(jnp.int32, (128, 256), 1)
        - 64
        - lax.broadcasted_iota(jnp.int32, (128, 256), 0)
    )
    band[...] = (
        ((delta + 1024) % 4 == 0) & (delta >= -4 * hw) & (delta <= 4 * hw - 4)
    ).astype(F32).astype(BF)

    for e in range(3):
        pos = lax.broadcasted_iota(jnp.int32, (512, 128), 0) // 4
        lo = pos - hw
        hi = pos + hw - 1
        if e == 1:
            lo = jnp.maximum(lo, 0)
        if e == 2:
            hi = jnp.minimum(hi, 127)
        inv[e] = 1.0 / (hi - lo + 1).astype(F32)

    for cp in wcopies[2:]:
        cp.wait()

    def prep(l, carry):
        rows = pl.ds(pl.multiple_of(l * 128, 128), 128)
        g = jnp.transpose(jnp.broadcast_to(gain[pl.ds(l, 1), :], (128, 128)))
        for t in (0, 1, 2, 4):
            cols = slice(128 * t, 128 * t + 128)
            wb[rows, cols] = (wb[rows, cols].astype(F32) * g).astype(BF)
        kv = jnp.transpose(kvt[:, rows].astype(F32))
        wb[rows, 384:512] = (kv * g).astype(BF)
        return carry

    lax.fori_loop(0, 16, prep, 0, unroll=2)

    qgain = jnp.concatenate([qg[...], qg[...]], axis=1) * (0.125 * LOG2E)
    kgain = jnp.concatenate([kg[...], kg[...]], axis=1)

    def halo(i, src, dst, dev):
        return remote(src, dst, hsend.at[i], hrecv.at[i], dev)

    def halo_left():
        return (
            halo(0, kvs.at[:, pl.ds(128, 128), :], kvs.at[:, pl.ds(9 * 128, 128), :], (sp - 1, tp)),
            halo(1, poolbuf.at[pl.ds(64, 32)], poolbuf.at[pl.ds(64 + 4096, 32)], (sp - 1, tp)),
        )

    def halo_right():
        return (
            halo(2, kvs.at[:, pl.ds(8 * 128, 128), :], kvs.at[:, pl.ds(0, 128), :], (sp + 1, tp)),
            halo(3, poolbuf.at[pl.ds(64 + 4096 - 32, 32)], poolbuf.at[pl.ds(32, 32)], (sp + 1, tp)),
        )

    def multiply(k):
        p = (pa, pc)[k % 2]
        x = (xa, xc)[k % 2][...].reshape(512, 2048)
        p[...] = jnp.dot(x, wb[...], preferred_element_type=F32)

    def ready(k):
        if COMM:
            blk = order(k)

            @pl.when(blk != tp)
            def _():
                rcopy(blk, blk).wait_recv()

    def finish(k):
        blk = order(k)
        p = (pa, pc)[k % 2]
        r = jnp.concatenate(
            [
                jnp.transpose(jnp.broadcast_to(rbuf[blk, g : g + 1, :], (128, 128)))
                for g in range(4)
            ],
            axis=0,
        )
        rows = pl.ds(pl.multiple_of(blk * 512, 512), 512)
        prows = pl.ds(pl.multiple_of(blk * 512 + 64, 64), 512)
        poolbuf[prows, :] = (p[:, 0:128] * r).astype(BF)
        gate[rows, :] = (p[:, 128:256] * r).astype(BF)
        agate[rows, :] = (p[:, 512:640] * r).astype(BF)
        q = (p[:, 256:384] * r).astype(BF).astype(F32)
        rq = lax.rsqrt(split_dot(q * q, head_ones) * (1.0 / 64) + EPS)
        tmp[0] = q * rq * qgain
        kv = (p[:, 384:512] * r).astype(BF).astype(F32)
        rk = lax.rsqrt(split_dot(kv * kv, head_ones) * (1.0 / 64) + EPS)
        tmp[1] = jnp.where(low, kv * rk * kgain, kv)
        for s in range(4):
            q = tmp[0, pl.ds(s, 128, stride=4), :]
            qs[blk, s, 0:128, :] = jnp.where(low, q, 0.0).astype(BF)
            qs[blk, s, 128:256, :] = jnp.where(low, pltpu.roll(q, 64, 1), 0.0).astype(BF)
            kvs[s, pl.ds(pl.multiple_of((blk + 1) * 128, 128), 128), :] = tmp[
                1, pl.ds(s, 128, stride=4), :
            ].astype(BF)

    def edges(k):
        if COMM:
            blk = order(k)

            @pl.when((blk == 0) & (sp > 0))
            def _():
                for cp in halo_left():
                    cp.start()

            @pl.when((blk == 7) & (sp < NSP - 1))
            def _():
                for cp in halo_right():
                    cp.start()

    def emit(part, blk):
        if COMM:
            @pl.when(blk != tp)
            def _():
                remote(
                    ysend.at[part, blk], yr.at[part, tp], asend.at[part, blk], arecv.at[part, tp], (sp, blk)
                ).start()

    def pool_wait(blk):
        if COMM:
            @pl.when((blk == 0) & (sp > 0))
            def _():
                halo_right()[1].wait_recv()

            @pl.when((blk == 7) & (sp < NSP - 1))
            def _():
                halo_left()[1].wait_recv()

    def pool(blk):
        start = pl.multiple_of(blk * 512, 512)
        sums = jnp.concatenate(
            [
                jnp.dot(band[...], poolbuf[pl.ds(start + 128 * g, 256), :], preferred_element_type=F32)
                for g in range(4)
            ],
            axis=0,
        )
        scale = inv[sp0 * (1 - (blk + 7) // 8) + 2 * sp15 * ((blk + 1) // 8)]
        own = poolbuf[pl.ds(start + 64, 512), :].astype(F32)
        pooled = (sums * scale - own).astype(BF)
        mixed = jnp.dot(pooled, mix[0], preferred_element_type=F32)
        g = gate[pl.ds(start, 512), :].astype(F32)
        ysend[0, blk] = (mixed * silu(g)).astype(BF)

    def step(k, top, pooling):
        if top:
            xcopy(k).wait()
        if k > 0:
            ready(k - 1)
        if pooling:
            pool_wait(order(k - 3))
        if top:
            multiply(k)
        if k > 0:
            finish(k - 1)
        if pooling:
            pool(order(k - 3))
        if top and k + 2 < 8:
            xcopy(k + 2).start()
        if k > 0:
            edges(k - 1)
        if pooling:
            emit(0, order(k - 3))

    for k in range(8):
        step(k, True, k >= 4)
        if COMM and k in (2, 4, 6):
            {2: event1, 4: event2, 6: event3}[k]()
    step(8, False, True)

    def pool_rest(k, carry):
        blk = order(k % 8)
        pool_wait(blk)
        pool(blk)
        emit(0, blk)
        return carry

    lax.fori_loop(6, 9, pool_rest, 0)

    def attend(blk):
        if COMM:
            @pl.when((blk == 0) & (sp > 0))
            def _():
                halo_right()[0].wait_recv()

            @pl.when((blk == 7) & (sp < NSP - 1))
            def _():
                halo_left()[0].wait_recv()

        left = 3 * sp0 * (1 - (blk + 7) // 8)
        right = 2 + sp15 * ((blk + 1) // 8)
        for s in range(4):
            q = qs[blk, s]
            kv = kvs[s, pl.ds(pl.multiple_of(blk * 128, 128), 384), :]
            scores = lax.dot_general(q, kv, (((1,), (1,)), ((), ())), preferred_element_type=F32)
            w = jnp.concatenate(
                [
                    jnp.exp2(scores[:, 128 * p : 128 * p + 128] + bias[at]).astype(BF)
                    for p, at in ((0, left), (1, 1), (2, right))
                ],
                axis=1,
            )
            rhs = jnp.concatenate([kv, jnp.ones((384, 128), BF)], axis=1)
            o = jnp.dot(w, rhs, preferred_element_type=F32)
            t0 = o[0:128, 128:256] + jnp.exp(jnp.full((1, 128), s0 - m0, F32))
            t1 = o[128:256, 128:256] + jnp.exp(jnp.full((1, 128), s1 - m1, F32))
            over = jnp.where(low, pltpu.roll(o[0:128, 0:128], 64, 1), o[128:256, 0:128])
            att[pl.ds(s, 128, stride=4), :] = over / jnp.where(low, t0, t1)
            totals = jnp.log(jnp.transpose(jnp.where(lane == 0, t0, t1))[0:2, :])
            top = jnp.where(lax.broadcasted_iota(jnp.int32, (2, 128), 0) == 0, m0, m1)
            lse[s, :, pl.ds(pl.multiple_of(blk * 128, 128), 128)] = top + totals
        g = agate[pl.ds(pl.multiple_of(blk * 512, 512), 512), :].astype(F32)
        ysend[1, blk] = (att[...] * silu(g)).astype(BF)
        emit(1, blk)

    def att_step(k, carry):
        j = k // 2
        d = (2 + 3 * j + 3 * (j // 2) + 2 * (j // 3)) % 4
        d = (d + c * (4 - 2 * d)) % 4
        attend(((chip + d) % 4) * 2 + (c + 1 + k) % 2)
        if COMM:
            for at, event in ((1, event4), (5, event5)):
                pl.when(k == at)(event)
        return carry

    lax.fori_loop(0, 8, att_step, 0)

    def exchange(part, j):
        return remote(
            ysend.at[part, j], yr.at[part, tp], asend.at[part, j], arecv.at[part, j], (sp, j)
        )

    def arrive(part):
        if COMM:
            for j in range(8):
                @pl.when(tp != j)
                def _():
                    remote(
                        ysend.at[part, j], yr.at[part, j], asend.at[part, j], arecv.at[part, j], (sp, j)
                    ).wait_recv()

    if COMM:
        for da in range(4):
            for db in range(4):
                if da or db:
                    ref = wg.at[1 - c, ((b_ + da) % 4) * sb + ((a + db) % 4) * sa]
                    remote(
                        ref, ref, dsend.at[da * 4 + db], drecv.at[da * 4 + db], (sp, tp + 1 - 2 * c)
                    ).wait_recv()

    for part in range(2):
        yr[part, tp] = ysend[part, tp]

    arrive(0)

    def out_pool_step(n, carry):
        cols = pl.ds(pl.multiple_of(n * 512, 512), 512)
        acts = jnp.concatenate([yr[0, j] for j in range(8)], axis=1)
        acc[:, cols] = jnp.dot(
            acts, wg[0, :, :, cols].reshape(1024, 512), preferred_element_type=F32
        )
        return carry

    lax.fori_loop(0, 4, out_pool_step, 0)
    arrive(1)

    def out_attn_step(n, carry):
        cols = pl.ds(pl.multiple_of(n * 512, 512), 512)
        acts = jnp.concatenate([yr[1, j] for j in range(8)], axis=1)
        total = acc[:, cols] + jnp.dot(
            acts, wg[1, :, :, cols].reshape(1024, 512), preferred_element_type=F32
        )
        out[:, :, cols] = total.astype(BF).reshape(128, 4, 512)
        return carry

    lax.fori_loop(0, 4, out_attn_step, 0)

    if COMM:
        for part in range(2):
            for j in range(8):
                @pl.when(tp != j)
                def _():
                    exchange(part, j).wait_send()
        for j in range(8):
            @pl.when(tp != j)
            def _():
                rcopy(j, tp).wait_send()
        for item in sends:
            gcopy(*item).wait_send()
        for da in range(4):
            for db in range(4):
                if da or db:
                    across(da, db).wait_send()

        @pl.when(sp > 0)
        def _():
            for cp in halo_left():
                cp.wait_send()

        @pl.when(sp < NSP - 1)
        def _():
            for cp in halo_right():
                cp.wait_send()


def layer(
    inputs, norm_gain, pool_proj, pool_gate_proj, pool_mix, query_proj, key_proj, value_proj,
    attn_gate_proj, query_gain, key_gain, sink_logit, out_pool, out_attn,
):
    hbm = pl.BlockSpec(memory_space=pl.ANY)
    vmem = pl.BlockSpec(memory_space=pltpu.VMEM)
    smem = pl.BlockSpec(memory_space=pltpu.SMEM)
    dma = pltpu.SemaphoreType.DMA
    mixed, log_sums = pl.pallas_call(
        kernel,
        out_shape=(
            jax.ShapeDtypeStruct((128, 4, 2048), BF),
            jax.ShapeDtypeStruct((4, 2, 1024), F32),
        ),
        in_specs=[hbm, vmem, hbm, hbm, hbm, hbm, hbm, hbm, vmem, vmem, vmem, smem, hbm, hbm],
        out_specs=(vmem, vmem),
        scratch_shapes=[
            pltpu.VMEM((128, 4, 2048), BF),
            pltpu.VMEM((128, 4, 2048), BF),
            pltpu.VMEM((128, 4, 2048), BF),
            pltpu.VMEM((2048, 640), BF),
            pltpu.VMEM((128, 2048), BF),
            pltpu.VMEM((512, 640), F32),
            pltpu.VMEM((512, 640), F32),
            pltpu.VMEM((2, 512, 128), F32),
            pltpu.VMEM((3, 512, 128), F32),
            pltpu.VMEM((8, 128), F32),
            pltpu.VMEM((8, 8, 128), F32),
            pltpu.VMEM((8, 4, 256, 128), BF),
            pltpu.VMEM((4, 1280, 128), BF),
            pltpu.VMEM((4096 + 128, 128), BF),
            pltpu.VMEM((4096, 128), BF),
            pltpu.VMEM((4096, 128), BF),
            pltpu.VMEM((4, 256, 128), F32),
            pltpu.VMEM((128, 256), BF),
            pltpu.VMEM((2, 8, 512, 128), BF),
            pltpu.VMEM((2, 8, 512, 128), BF),
            pltpu.VMEM((2, 16, 64, 2048), BF),
            pltpu.VMEM((512, 2048), F32),
            pltpu.VMEM((512, 128), F32),
            dma((3,)), dma((8,)), dma((8,)), dma((8,)),
            dma((2, 8)), dma((2, 8)),
            dma((4,)), dma((4,)),
            dma((24,)), dma((16, 2)),
            dma((16,)), dma((16,)),
        ],
        compiler_params=pltpu.CompilerParams(
            vmem_limit_bytes=60 * 1024 * 1024,
            **(dict(collective_id=0, has_side_effects=True) if COMM else {}),
        ),
        name="mixer_layer",
    )(
        inputs, norm_gain.reshape(16, 128), pool_proj, pool_gate_proj, query_proj, key_proj.T,
        value_proj.T, attn_gate_proj, pool_mix, query_gain.reshape(1, 64), key_gain.reshape(1, 64),
        sink_logit, out_pool, out_attn,
    )
    return mixed, jnp.transpose(log_sums, (2, 0, 1))


def solution(mesh):
    placed = (
        P("sp", None, None), P(), P(None, "tp"), P(None, "tp"), P("tp", None, None), P(None, "tp"),
        P(None, "tp"), P(None, "tp"), P(None, "tp"), P(), P(), P("tp"), P("sp", None), P("sp", None),
    )
    return jax.shard_map(
        layer,
        mesh=mesh,
        in_specs=placed,
        out_specs=(P(("sp", "tp"), None, None), P("sp", None, "tp")),
        check_vma=False,
    )
```

```python
import functools

import jax
import jax.numpy as jnp
from jax import lax
from jax.experimental import pallas as pl
from jax.experimental.pallas import tpu as pltpu
from jax.sharding import PartitionSpec as P

HEADS = 16
EPS = 1e-06
NEG = -1e30
SHIFT = 29.5
LOG2E = 1.4426950408889634
BF = jnp.bfloat16
F32 = jnp.float32
SEQ_LEN = 16384
NSP = 16
COMM = True
NEAR = (0, 2)
FAR = (1, 3)


def split_dot(values, ones):
    hi = values.astype(BF)
    lo = (values - hi.astype(F32)).astype(BF)
    return jnp.dot(hi, ones, preferred_element_type=F32) + jnp.dot(lo, ones, preferred_element_type=F32)


def silu(v):
    return v / (1.0 + jnp.exp(-v))


def kernel(
    x_hbm, gain, pw, gw, qw, kw, vw, aw, mix, qg, kg, sink, outp, outa,
    out, lse,
    xa, xc, xo, xe, edge, wb, kvt, pa, pc, tmp, inv, rsend, rbuf, qs, kvs, poolbuf, gate, agate, bias, band, ysend, yr, wg, acc, att, relay,
    xsem, wsem, rs_send, rs_recv, lsend, lrecv, asend, arecv, hsend, hrecv, gsend, grecv, dsend, drecv,
):
    if COMM:
        sp = lax.axis_index("sp")
        tp = lax.axis_index("tp")
    else:
        sp = jnp.int32(0)
        tp = jnp.int32(0)
    chip = tp // 2
    c = tp % 2
    y = sp % 4
    z = sp // 4
    a = y * (1 - c) + z * c
    b_ = z * (1 - c) + y * c
    sa = 1 + 3 * c
    sb = 4 - 3 * c

    def order(k):
        return (2 * chip + 1 - c + (k + 2) - 2 * c * (k + 2) + 16) % 8

    def xcopy(k):
        return pltpu.make_async_copy(
            x_hbm.at[pl.ds(order(k) * 128, 128)], (xa, xc)[k % 2], xsem.at[k % 2]
        )

    xown = pltpu.make_async_copy(x_hbm.at[pl.ds(tp * 128, 128)], xo, xsem.at[2])
    xown.start()
    xedge = (
        pltpu.make_async_copy(x_hbm.at[pl.ds(0, 8)], xe.at[pl.ds(0, 8)], xsem.at[3]),
        pltpu.make_async_copy(x_hbm.at[pl.ds(1016, 8)], xe.at[pl.ds(8, 8)], xsem.at[4]),
    )
    for cp in xedge:
        cp.start()

    wcopies = [
        pltpu.make_async_copy(outp, wg.at[0, sp], wsem.at[0]),
        pltpu.make_async_copy(outa, wg.at[1, sp], wsem.at[1]),
        pltpu.make_async_copy(pw, wb.at[:, pl.ds(0, 128)], wsem.at[2]),
        pltpu.make_async_copy(gw, wb.at[:, pl.ds(128, 128)], wsem.at[3]),
        pltpu.make_async_copy(qw, wb.at[:, pl.ds(256, 128)], wsem.at[4]),
        pltpu.make_async_copy(kw, kvt.at[pl.ds(0, 64)], wsem.at[5]),
        pltpu.make_async_copy(vw, kvt.at[pl.ds(64, 64)], wsem.at[6]),
        pltpu.make_async_copy(aw, wb.at[:, pl.ds(512, 128)], wsem.at[7]),
    ]
    for cp in wcopies:
        cp.start()
    xcopy(0).start()
    xcopy(1).start()

    zeros = jnp.zeros((64, 128), BF)
    poolbuf[0:64, :] = zeros
    poolbuf[64 + 4096 : 128 + 4096, :] = zeros
    for s in range(4):
        kvs[s, 0:128, :] = jnp.zeros((128, 128), BF)
        kvs[s, 9 * 128 : 10 * 128, :] = jnp.zeros((128, 128), BF)

    def remote(src, dst, ss, rs, dev):
        return pltpu.make_async_remote_copy(
            src_ref=src, dst_ref=dst, send_sem=ss, recv_sem=rs,
            device_id=dev, device_id_type=pl.DeviceIdType.MESH,
        )

    if COMM:
        barrier = pltpu.get_barrier_semaphore()

        def greet(dev):
            pl.semaphore_signal(barrier, inc=1, device_id=dev, device_id_type=pl.DeviceIdType.MESH)

        for j in range(1, 8):
            greet((sp, (tp + j) % 8))
        greet((z * 4 + (y + 1) % 4, tp))
        greet((z * 4 + (y + 3) % 4, tp))
        greet((((z + 1) % 4) * 4 + y, tp))
        greet((((z + 3) % 4) * 4 + y, tp))

        greet(((sp + 1) % NSP, tp))
        greet(((sp + NSP - 1) % NSP, tp))

    sp0 = 1 - (sp + 15) // 16
    sp15 = (sp + 1) // 16

    def slice_at(da, db):
        return ((a + da) % 4) * sa + ((b_ + db) % 4) * sb

    def piece(da, db, half):
        if half is None:
            return wg.at[c, slice_at(da, db)]
        return wg.at[c, slice_at(da, db), pl.ds(32 * half, 32)]

    sends = []

    def gcopy(da, db, half, ma, mb, n):
        return remote(
            piece(da, db, half), piece(da, db, half), gsend.at[n],
            grecv.at[((da - ma) % 4) * 4 + (db - mb) % 4, half or 0],
            (slice_at(ma, mb), tp),
        )

    def send(da, db, half, ma, mb):
        if COMM:
            n = len(sends)
            sends.append((da, db, half, ma, mb, n))
            gcopy(da, db, half, ma, mb, n).start()

    def got(da, db, half=None):
        if COMM:
            ref = piece(da, db, half)
            remote(
                ref, ref, gsend.at[0], grecv.at[da * 4 + db, half or 0], (sp, tp + 1 - 2 * c)
            ).wait_recv()

    def across(da, db):
        ref = piece(da, db, None)
        return remote(
            ref, ref, dsend.at[da * 4 + db], drecv.at[da * 4 + db], (sp, tp + 1 - 2 * c)
        )

    def share(da, db):
        if COMM:
            across(da, db).start()

    def event0():
        send(0, 0, None, 1, 0)
        send(0, 0, None, -1, 0)
        send(0, 0, None, 0, 1)
        send(0, 0, None, 0, -1)

    def event1():
        got(3, 0)
        send(3, 0, 0, 1, 0)
        got(1, 0)
        send(1, 0, 1, -1, 0)
        for da in (3, 1):
            send(da, 0, None, 0, 1)
            send(da, 0, None, 0, -1)
            share(da, 0)

    def through(da):
        got(da, 3)
        send(da, 3, 0, 0, 1)
        share(da, 3)
        got(da, 1)
        send(da, 1, 1, 0, -1)
        share(da, 1)

    def far(da):
        got(da, 2, 0)
        got(da, 2, 1)
        share(da, 2)

    def event2():
        got(2, 0, 0)
        got(2, 0, 1)
        send(2, 0, None, 0, 1)
        send(2, 0, None, 0, -1)
        share(2, 0)
        through(0)

    def event3():
        through(3)
        through(1)
        far(0)

    def event4():
        through(2)

    def event5():
        far(3)
        far(1)

    def event6():
        far(2)

    lane = lax.broadcasted_iota(jnp.int32, (1, 128), 1)
    low = lane < 64
    ones = jnp.ones((128, 128), BF)
    row128 = lax.broadcasted_iota(jnp.int32, (128, 128), 0)
    col128 = lax.broadcasted_iota(jnp.int32, (128, 128), 1)
    head_ones = ((row128 // 64) == (col128 // 64)).astype(F32).astype(BF)

    tpf = tp.astype(F32)
    s0 = sink[0]
    s1 = sink[1]
    m0 = jnp.maximum(s0, SHIFT)
    m1 = jnp.maximum(s1, SHIFT)
    for h in range(2):
        slope = jnp.exp2(jnp.full((128, 128), -(2.0 * tpf + (h + 1.0)) * 0.5, F32))
        m = (m0, m1)[h]
        for p in range(3):
            i = lax.broadcasted_iota(jnp.int32, (128, 128), 0)
            j = lax.broadcasted_iota(jnp.int32, (128, 128), 1)
            dist = jnp.abs(i - j - (128 * p - 128))
            val = (-slope * dist.astype(F32) - m) * LOG2E
            bias[p, 128 * h : 128 * h + 128, :] = jnp.where(dist <= 128, val, NEG)
        bias[3, 128 * h : 128 * h + 128, :] = jnp.full((128, 128), NEG, F32)

    hw = jnp.left_shift(jnp.int32(1), tp % 4)
    delta = (
        lax.broadcasted_iota(jnp.int32, (128, 256), 1)
        - 64
        - lax.broadcasted_iota(jnp.int32, (128, 256), 0)
    )
    band[...] = (
        ((delta + 1024) % 4 == 0) & (delta >= -4 * hw) & (delta <= 4 * hw - 4)
    ).astype(F32).astype(BF)

    for e in range(3):
        pos = lax.broadcasted_iota(jnp.int32, (512, 128), 0) // 4
        lo = pos - hw
        hi = pos + hw - 1
        if e == 1:
            lo = jnp.maximum(lo, 0)
        if e == 2:
            hi = jnp.minimum(hi, 127)
        inv[e] = 1.0 / (hi - lo + 1).astype(F32)

    if COMM:
        pl.semaphore_wait(barrier, 13)

    wcopies[0].wait()
    wcopies[1].wait()
    event0()

    def row_scale(x):
        sq = jnp.zeros((x.shape[0], 128), F32)
        for l in range(16):
            t = x[:, 128 * l : 128 * l + 128].astype(F32)
            sq = sq + t * t
        return lax.rsqrt(split_dot(sq, ones) * (1.0 / 2048) + EPS)

    xown.wait()
    r = row_scale(xo[...].reshape(512, 2048))
    packed = [
        jnp.sum(jnp.where(row128 == col128, r[128 * g : 128 * g + 128], 0.0), axis=0, keepdims=True)
        for g in range(4)
    ]
    packed = jnp.concatenate(packed + [jnp.zeros((4, 128), F32)], axis=0)
    rsend[...] = packed
    rbuf[tp] = packed

    def rcopy(j, at):
        return remote(rsend, rbuf.at[at], rs_send.at[j], rs_recv.at[at], (sp, j))

    if COMM:
        for j in range(8):
            @pl.when(tp != j)
            def _():
                rcopy(j, tp).start()


    for cp in wcopies[2:]:
        cp.wait()

    def prep(l, carry):
        rows = pl.ds(pl.multiple_of(l * 128, 128), 128)
        g = jnp.transpose(jnp.broadcast_to(gain[pl.ds(l, 1), :], (128, 128)))
        for t in (0, 1, 2, 4):
            cols = slice(128 * t, 128 * t + 128)
            wb[rows, cols] = (wb[rows, cols].astype(F32) * g).astype(BF)
        kv = jnp.transpose(kvt[:, rows].astype(F32))
        wb[rows, 384:512] = (kv * g).astype(BF)
        return carry

    lax.fori_loop(0, 16, prep, 0, unroll=2)

    qgain = jnp.concatenate([qg[...], qg[...]], axis=1) * (0.125 * LOG2E)
    kgain = jnp.concatenate([kg[...], kg[...]], axis=1)

    def halo(i, src, dst, dev):
        return remote(src, dst, hsend.at[i], hrecv.at[i], dev)

    def halo_left():
        return (
            halo(0, kvs.at[:, pl.ds(128, 128), :], kvs.at[:, pl.ds(9 * 128, 128), :], (sp - 1, tp)),
            halo(1, edge.at[pl.ds(0, 32)], poolbuf.at[pl.ds(64 + 4096, 32)], (sp - 1, tp)),
        )

    def halo_right():
        return (
            halo(2, kvs.at[:, pl.ds(8 * 128, 128), :], kvs.at[:, pl.ds(0, 128), :], (sp + 1, tp)),
            halo(3, edge.at[pl.ds(32, 32)], poolbuf.at[pl.ds(32, 32)], (sp + 1, tp)),
        )

    for cp in xedge:
        cp.wait()
    x = xe[...].reshape(64, 2048)
    edge[...] = (
        jnp.dot(x, wb[:, 0:128], preferred_element_type=F32) * row_scale(x)
    ).astype(BF)
    if COMM:
        @pl.when(sp > 0)
        def _():
            halo_left()[1].start()

        @pl.when(sp < NSP - 1)
        def _():
            halo_right()[1].start()

    def multiply(k, lo, hi):
        p = (pa, pc)[k % 2]
        x = (xa, xc)[k % 2][...].reshape(512, 2048)
        p[:, lo:hi] = jnp.dot(x, wb[:, lo:hi], preferred_element_type=F32)

    def ready(k):
        if COMM:
            blk = order(k)

            @pl.when(blk != tp)
            def _():
                rcopy(blk, blk).wait_recv()

    def scales(k):
        blk = order(k)
        return jnp.concatenate(
            [
                jnp.transpose(jnp.broadcast_to(rbuf[blk, g : g + 1, :], (128, 128)))
                for g in range(4)
            ],
            axis=0,
        )

    def finish_gates(k, r):
        blk = order(k)
        p = (pa, pc)[k % 2]
        rows = pl.ds(pl.multiple_of(blk * 512, 512), 512)
        prows = pl.ds(pl.multiple_of(blk * 512 + 64, 64), 512)
        poolbuf[prows, :] = (p[:, 0:128] * r).astype(BF)
        gate[rows, :] = (p[:, 128:256] * r).astype(BF)
        agate[rows, :] = (p[:, 512:640] * r).astype(BF)

    def finish_heads(k, r):
        blk = order(k)
        p = (pa, pc)[k % 2]
        q = (p[:, 256:384] * r).astype(BF).astype(F32)
        rq = lax.rsqrt(split_dot(q * q, head_ones) * (1.0 / 64) + EPS)
        tmp[0] = q * rq * qgain
        kv = (p[:, 384:512] * r).astype(BF).astype(F32)
        rk = lax.rsqrt(split_dot(kv * kv, head_ones) * (1.0 / 64) + EPS)
        tmp[1] = jnp.where(low, kv * rk * kgain, kv)
        for s in range(4):
            q = tmp[0, pl.ds(s, 128, stride=4), :]
            qs[blk, s, 0:128, :] = jnp.where(low, q, 0.0).astype(BF)
            qs[blk, s, 128:256, :] = jnp.where(low, pltpu.roll(q, 64, 1), 0.0).astype(BF)
            kvs[s, pl.ds(pl.multiple_of((blk + 1) * 128, 128), 128), :] = tmp[
                1, pl.ds(s, 128, stride=4), :
            ].astype(BF)

    def edges(k):
        if COMM:
            blk = order(k)

            @pl.when((blk == 0) & (sp > 0))
            def _():
                halo_left()[0].start()

            @pl.when((blk == 7) & (sp < NSP - 1))
            def _():
                halo_right()[0].start()

    def ahead(part):
        return (chip + 1 + 2 * ((c + part) % 2)) % 4

    def behind(part):
        return ((chip + 3 + 2 * ((c + part) % 2)) % 4) * 2 + c

    def direct(part, blk):
        return remote(
            ysend.at[part, blk], yr.at[part, tp], asend.at[part, blk], arecv.at[part, tp], (sp, blk)
        )

    def first_hop(part, blk):
        return remote(
            ysend.at[part, blk], relay.at[part, blk % 2], asend.at[part, blk], lrecv.at[part, blk % 2],
            (sp, ahead(part) * 2 + c),
        )

    def second_hop(part, e):
        return remote(
            relay.at[part, e], yr.at[part, behind(part)], lsend.at[part, e], arecv.at[part, behind(part)],
            (sp, ahead(part) * 2 + e),
        )

    def away(blk):
        return (blk // 2 - chip + 4) % 4

    def emit(part, blk):
        if COMM:
            @pl.when((blk != tp) & (away(blk) != 2))
            def _():
                direct(part, blk).start()

            @pl.when(away(blk) == 2)
            def _():
                first_hop(part, blk).start()

    def pass_on(part, e):
        if COMM:
            first_hop(part, e).wait_recv()
            second_hop(part, e).start()

    def pool_wait(blk):
        if COMM:
            @pl.when((blk == 0) & (sp > 0))
            def _():
                halo_right()[1].wait_recv()

            @pl.when((blk == 7) & (sp < NSP - 1))
            def _():
                halo_left()[1].wait_recv()

    def pool(blk):
        start = pl.multiple_of(blk * 512, 512)
        sums = jnp.concatenate(
            [
                jnp.dot(band[...], poolbuf[pl.ds(start + 128 * g, 256), :], preferred_element_type=F32)
                for g in range(4)
            ],
            axis=0,
        )
        scale = inv[sp0 * (1 - (blk + 7) // 8) + 2 * sp15 * ((blk + 1) // 8)]
        own = poolbuf[pl.ds(start + 64, 512), :].astype(F32)
        pooled = (sums * scale - own).astype(BF)
        mixed = jnp.dot(pooled, mix[0], preferred_element_type=F32)
        g = gate[pl.ds(start, 512), :].astype(F32)
        ysend[0, blk] = (mixed * silu(g)).astype(BF)

    def step(k, top, pooling):
        if top:
            xcopy(k).wait()
        if k > 0:
            ready(k - 1)
        if pooling:
            pool_wait(order(k - 2))
        if top:
            multiply(k, 0, 256)
        if k > 0:
            r = scales(k - 1)
            finish_gates(k - 1, r)
        if top:
            multiply(k, 256, 512)
        if k > 0:
            finish_heads(k - 1, r)
        if top:
            multiply(k, 512, 640)
        if pooling:
            pool(order(k - 2))
        if top and k + 2 < 8:
            xcopy(k + 2).start()
        if k > 0:
            edges(k - 1)
        if pooling:
            emit(0, order(k - 2))

    for k in range(8):
        step(k, True, k >= 3)
        if k == 1:
            event1()
        if k == 3:
            event2()
        if k == 6:
            event3()
        if k == 5:
            pass_on(0, c)
        if k == 6:
            pass_on(0, 1 - c)
    step(8, False, True)

    def pool_rest(k, carry):
        blk = order(k % 8)
        pool_wait(blk)
        pool(blk)
        emit(0, blk)
        return carry

    lax.fori_loop(7, 9, pool_rest, 0)
    event4()

    def attend(blk):
        if COMM:
            @pl.when((blk == 0) & (sp > 0))
            def _():
                halo_right()[0].wait_recv()

            @pl.when((blk == 7) & (sp < NSP - 1))
            def _():
                halo_left()[0].wait_recv()

        left = 3 * sp0 * (1 - (blk + 7) // 8)
        right = 2 + sp15 * ((blk + 1) // 8)
        for s in range(4):
            q = qs[blk, s]
            kv = kvs[s, pl.ds(pl.multiple_of(blk * 128, 128), 384), :]
            scores = lax.dot_general(q, kv, (((1,), (1,)), ((), ())), preferred_element_type=F32)
            w = jnp.concatenate(
                [
                    jnp.exp2(scores[:, 128 * p : 128 * p + 128] + bias[at]).astype(BF)
                    for p, at in ((0, left), (1, 1), (2, right))
                ],
                axis=1,
            )
            rhs = jnp.concatenate([kv, jnp.ones((384, 128), BF)], axis=1)
            o = jnp.dot(w, rhs, preferred_element_type=F32)
            t0 = o[0:128, 128:256] + jnp.exp(jnp.full((1, 128), s0 - m0, F32))
            t1 = o[128:256, 128:256] + jnp.exp(jnp.full((1, 128), s1 - m1, F32))
            over = jnp.where(low, pltpu.roll(o[0:128, 0:128], 64, 1), o[128:256, 0:128])
            att[pl.ds(s, 128, stride=4), :] = over / jnp.where(low, t0, t1)
            totals = jnp.log(jnp.transpose(jnp.where(lane == 0, t0, t1))[0:2, :])
            top = jnp.where(lax.broadcasted_iota(jnp.int32, (2, 128), 0) == 0, m0, m1)
            lse[s, :, pl.ds(pl.multiple_of(blk * 128, 128), 128)] = top + totals
        g = agate[pl.ds(pl.multiple_of(blk * 512, 512), 512), :].astype(F32)
        ysend[1, blk] = (att[...] * silu(g)).astype(BF)
        emit(1, blk)

    def att_step(k, carry):
        j = k // 2
        d = (2 + 3 * j + 3 * (j // 2) + 2 * (j // 3)) % 4
        d = (d + c * (4 - 2 * d)) % 4
        attend(((chip + d) % 4) * 2 + (c + 1 + k) % 2)
        if COMM:
            for at, event in (
                (3, event5),
                (4, functools.partial(pass_on, 1, (c + 1) % 2)),
                (5, event6),
                (6, functools.partial(pass_on, 1, c)),
            ):
                pl.when(k == at)(event)
        return carry

    lax.fori_loop(0, 8, att_step, 0)

    def arrive(part, j):
        if COMM:
            @pl.when(tp != j)
            def _():
                remote(
                    ysend.at[part, j], yr.at[part, j], asend.at[part, j], arecv.at[part, j], (sp, j)
                ).wait_recv()

    if COMM:
        for da in range(4):
            for db in range(4):
                if da or db:
                    ref = wg.at[1 - c, ((b_ + da) % 4) * sb + ((a + db) % 4) * sa]
                    remote(
                        ref, ref, dsend.at[da * 4 + db], drecv.at[da * 4 + db], (sp, tp + 1 - 2 * c)
                    ).wait_recv()

    for part in range(2):
        yr[part, tp] = ysend[part, tp]

    for j in range(8):
        arrive(0, j)

    def out_pool_step(n, carry):
        cols = pl.ds(pl.multiple_of(n * 512, 512), 512)
        acts = jnp.concatenate([yr[0, j] for j in range(8)], axis=1)
        acc[:, cols] = jnp.dot(
            acts, wg[0, :, :, cols].reshape(1024, 512), preferred_element_type=F32
        )
        return carry

    lax.fori_loop(0, 4, out_pool_step, 0)

    def attn_part(cols, d):
        src = [(chip + e) % 4 for e in d]
        acts = jnp.concatenate([yr[1, 2 * e + h] for e in src for h in range(2)], axis=1)
        rows = jnp.concatenate([wg[1, pl.ds(4 * e, 4), :, cols].reshape(256, 512) for e in src], axis=0)
        return acc[:, cols] + jnp.dot(acts, rows, preferred_element_type=F32)

    def out_near_step(n, carry):
        cols = pl.ds(pl.multiple_of(n * 512, 512), 512)
        acc[:, cols] = attn_part(cols, NEAR)
        return carry

    def out_attn_step(n, carry):
        cols = pl.ds(pl.multiple_of(n * 512, 512), 512)
        out[:, :, cols] = attn_part(cols, FAR).astype(BF).reshape(128, 4, 512)
        return carry

    for d in NEAR:
        for h in range(2):
            arrive(1, 2 * ((chip + d) % 4) + h)
    lax.fori_loop(0, 4, out_near_step, 0)
    for d in FAR:
        for h in range(2):
            arrive(1, 2 * ((chip + d) % 4) + h)
    lax.fori_loop(0, 4, out_attn_step, 0)

    if COMM:
        for part in range(2):
            for j in range(8):
                @pl.when(tp != j)
                def _():
                    direct(part, j).wait_send()
        for j in range(8):
            @pl.when(tp != j)
            def _():
                rcopy(j, tp).wait_send()
        for part in range(2):
            for e in range(2):
                second_hop(part, e).wait_send()
        for item in sends:
            gcopy(*item).wait_send()
        for da in range(4):
            for db in range(4):
                if da or db:
                    across(da, db).wait_send()

        @pl.when(sp > 0)
        def _():
            for cp in halo_left():
                cp.wait_send()

        @pl.when(sp < NSP - 1)
        def _():
            for cp in halo_right():
                cp.wait_send()


def layer(
    inputs, norm_gain, pool_proj, pool_gate_proj, pool_mix, query_proj, key_proj, value_proj,
    attn_gate_proj, query_gain, key_gain, sink_logit, out_pool, out_attn,
):
    hbm = pl.BlockSpec(memory_space=pl.ANY)
    vmem = pl.BlockSpec(memory_space=pltpu.VMEM)
    smem = pl.BlockSpec(memory_space=pltpu.SMEM)
    dma = pltpu.SemaphoreType.DMA
    mixed, log_sums = pl.pallas_call(
        kernel,
        out_shape=(
            pltpu.VMEM((128, 4, 2048), BF),
            pltpu.VMEM((4, 2, 1024), F32),
        ),
        in_specs=[hbm, vmem, hbm, hbm, hbm, hbm, hbm, hbm, vmem, vmem, vmem, smem, hbm, hbm],
        out_specs=(vmem, vmem),
        scratch_shapes=[
            pltpu.VMEM((128, 4, 2048), BF),
            pltpu.VMEM((128, 4, 2048), BF),
            pltpu.VMEM((128, 4, 2048), BF),
            pltpu.VMEM((16, 4, 2048), BF),
            pltpu.VMEM((64, 128), BF),
            pltpu.VMEM((2048, 640), BF),
            pltpu.VMEM((128, 2048), BF),
            pltpu.VMEM((512, 640), F32),
            pltpu.VMEM((512, 640), F32),
            pltpu.VMEM((2, 512, 128), F32),
            pltpu.VMEM((3, 512, 128), F32),
            pltpu.VMEM((8, 128), F32),
            pltpu.VMEM((8, 8, 128), F32),
            pltpu.VMEM((8, 4, 256, 128), BF),
            pltpu.VMEM((4, 1280, 128), BF),
            pltpu.VMEM((4096 + 128, 128), BF),
            pltpu.VMEM((4096, 128), BF),
            pltpu.VMEM((4096, 128), BF),
            pltpu.VMEM((4, 256, 128), F32),
            pltpu.VMEM((128, 256), BF),
            pltpu.VMEM((2, 8, 512, 128), BF),
            pltpu.VMEM((2, 8, 512, 128), BF),
            pltpu.VMEM((2, 16, 64, 2048), BF),
            pltpu.VMEM((512, 2048), F32),
            pltpu.VMEM((512, 128), F32),
            pltpu.VMEM((2, 2, 512, 128), BF),
            dma((5,)), dma((8,)), dma((8,)), dma((8,)), dma((2, 2)), dma((2, 2)),
            dma((2, 8)), dma((2, 8)),
            dma((4,)), dma((4,)),
            dma((24,)), dma((16, 2)),
            dma((16,)), dma((16,)),
        ],
        compiler_params=pltpu.CompilerParams(
            vmem_limit_bytes=60 * 1024 * 1024,
            **(dict(collective_id=0, has_side_effects=True) if COMM else {}),
        ),
        name="mixer_layer",
    )(
        inputs, norm_gain.reshape(16, 128), pool_proj, pool_gate_proj, query_proj, key_proj.T,
        value_proj.T, attn_gate_proj, pool_mix, query_gain.reshape(1, 64), key_gain.reshape(1, 64),
        sink_logit, out_pool, out_attn,
    )
    return mixed, jnp.transpose(log_sums, (2, 0, 1))


def solution(mesh):
    placed = (
        P("sp", None, None), P(), P(None, "tp"), P(None, "tp"), P("tp", None, None), P(None, "tp"),
        P(None, "tp"), P(None, "tp"), P(None, "tp"), P(), P(), P("tp"), P("sp", None), P("sp", None),
    )
    return jax.shard_map(
        layer,
        mesh=mesh,
        in_specs=placed,
        out_specs=(P(("sp", "tp"), None, None), P("sp", None, "tp")),
        check_vma=False,
    )
```

```python
import functools

import jax
import jax.numpy as jnp
from jax import lax
from jax.experimental import pallas as pl
from jax.experimental.pallas import tpu as pltpu
from jax.sharding import PartitionSpec as P

HEADS = 16
EPS = 1e-06
NEG = -1e30
SHIFT = 29.5
LOG2E = 1.4426950408889634
BF = jnp.bfloat16
F32 = jnp.float32
SEQ_LEN = 16384
NSP = 16
COMM = True
NEAR = (0, 2)
EARLY = {5: 1, 6: 3, 7: 2, 8: 4}
OWN = 5
FAR = (1, 3)


def split_dot(values, ones):
    hi = values.astype(BF)
    lo = (values - hi.astype(F32)).astype(BF)
    return jnp.dot(hi, ones, preferred_element_type=F32) + jnp.dot(lo, ones, preferred_element_type=F32)


def silu(v):
    return v / (1.0 + jnp.exp(-v))


def kernel(
    x_hbm, gain, pw, gw, qw, kw, vw, aw, mix, qg, kg, sink, outp, outa,
    out, lse,
    xb, xe, edge, rcol, wb, kvt, pa, pc, tmp, inv, rsend, rbuf, qs, kvs, poolbuf, gate, agate, bias, band, ysend, yr, wg, acc, att, relay,
    xsem, wsem, rs_send, rs_recv, lsend, lrecv, asend, arecv, hsend, hrecv, gsend, grecv, dsend, drecv,
):
    if COMM:
        sp = lax.axis_index("sp")
        tp = lax.axis_index("tp")
    else:
        sp = jnp.int32(0)
        tp = jnp.int32(0)
    chip = tp // 2
    c = tp % 2
    y = sp % 4
    z = sp // 4
    a = y * (1 - c) + z * c
    b_ = z * (1 - c) + y * c
    sa = 1 + 3 * c
    sb = 4 - 3 * c

    def order(k):
        return (2 * chip + 1 - c + (k + 2) - 2 * c * (k + 2) + 16) % 8

    def xcopy(k):
        return pltpu.make_async_copy(
            x_hbm.at[pl.ds(order(k) * 128, 128)], xb.at[order(k)], xsem.at[k]
        )

    xedge = (
        pltpu.make_async_copy(x_hbm.at[pl.ds(0, 8)], xe.at[pl.ds(0, 8)], xsem.at[8]),
        pltpu.make_async_copy(x_hbm.at[pl.ds(1016, 8)], xe.at[pl.ds(8, 8)], xsem.at[9]),
    )

    wcopies = [
        pltpu.make_async_copy(outp, wg.at[0, sp], wsem.at[0]),
        pltpu.make_async_copy(outa, wg.at[1, sp], wsem.at[1]),
        pltpu.make_async_copy(pw, wb.at[:, pl.ds(0, 128)], wsem.at[2]),
        pltpu.make_async_copy(gw, wb.at[:, pl.ds(128, 128)], wsem.at[3]),
        pltpu.make_async_copy(qw, wb.at[:, pl.ds(256, 128)], wsem.at[4]),
        pltpu.make_async_copy(kw, kvt.at[pl.ds(0, 64)], wsem.at[5]),
        pltpu.make_async_copy(vw, kvt.at[pl.ds(64, 64)], wsem.at[6]),
        pltpu.make_async_copy(aw, wb.at[:, pl.ds(512, 128)], wsem.at[7]),
    ]
    for cp in wcopies[:2]:
        cp.start()
    xcopy(OWN).start()
    for cp in wcopies[2:]:
        cp.start()
    for cp in xedge:
        cp.start()

    zeros = jnp.zeros((64, 128), BF)
    poolbuf[0:64, :] = zeros
    poolbuf[64 + 4096 : 128 + 4096, :] = zeros
    for s in range(4):
        kvs[s, 0:128, :] = jnp.zeros((128, 128), BF)
        kvs[s, 9 * 128 : 10 * 128, :] = jnp.zeros((128, 128), BF)

    def remote(src, dst, ss, rs, dev):
        return pltpu.make_async_remote_copy(
            src_ref=src, dst_ref=dst, send_sem=ss, recv_sem=rs,
            device_id=dev, device_id_type=pl.DeviceIdType.MESH,
        )

    if COMM:
        barrier = pltpu.get_barrier_semaphore()

        def greet(dev):
            pl.semaphore_signal(barrier, inc=1, device_id=dev, device_id_type=pl.DeviceIdType.MESH)

        for j in range(1, 8):
            greet((sp, (tp + j) % 8))
        greet((z * 4 + (y + 1) % 4, tp))
        greet((z * 4 + (y + 3) % 4, tp))
        greet((((z + 1) % 4) * 4 + y, tp))
        greet((((z + 3) % 4) * 4 + y, tp))

        greet(((sp + 1) % NSP, tp))
        greet(((sp + NSP - 1) % NSP, tp))

    sp0 = 1 - (sp + 15) // 16
    sp15 = (sp + 1) // 16

    def slice_at(da, db):
        return ((a + da) % 4) * sa + ((b_ + db) % 4) * sb

    def piece(da, db, half):
        if half is None:
            return wg.at[c, slice_at(da, db)]
        return wg.at[c, slice_at(da, db), pl.ds(32 * half, 32)]

    sends = []

    def gcopy(da, db, half, ma, mb, n):
        return remote(
            piece(da, db, half), piece(da, db, half), gsend.at[n],
            grecv.at[((da - ma) % 4) * 4 + (db - mb) % 4, half or 0],
            (slice_at(ma, mb), tp),
        )

    def send(da, db, half, ma, mb):
        if COMM:
            n = len(sends)
            sends.append((da, db, half, ma, mb, n))
            gcopy(da, db, half, ma, mb, n).start()

    def got(da, db, half=None):
        if COMM:
            ref = piece(da, db, half)
            remote(
                ref, ref, gsend.at[0], grecv.at[da * 4 + db, half or 0], (sp, tp + 1 - 2 * c)
            ).wait_recv()

    def across(da, db):
        ref = piece(da, db, None)
        return remote(
            ref, ref, dsend.at[da * 4 + db], drecv.at[da * 4 + db], (sp, tp + 1 - 2 * c)
        )

    def share(da, db):
        if COMM:
            across(da, db).start()

    def event0():
        send(0, 0, None, 1, 0)
        send(0, 0, None, -1, 0)

    def event0_late():
        send(0, 0, None, 0, 1)
        send(0, 0, None, 0, -1)

    def through(da):
        got(da, 3)
        send(da, 3, 0, 0, 1)
        share(da, 3)
        got(da, 1)
        send(da, 1, 1, 0, -1)
        share(da, 1)

    def far(da):
        got(da, 2, 0)
        got(da, 2, 1)
        share(da, 2)

    def event1():
        got(3, 0)
        send(3, 0, 0, 1, 0)
        got(1, 0)
        send(1, 0, 1, -1, 0)
        through(0)
        for da in (3, 1):
            send(da, 0, None, 0, 1)
            send(da, 0, None, 0, -1)
            share(da, 0)

    def event2():
        got(2, 0, 0)
        got(2, 0, 1)
        send(2, 0, None, 0, 1)
        send(2, 0, None, 0, -1)
        share(2, 0)

    def event3():
        through(3)
        through(1)

    def event4():
        through(2)

    def event5():
        far(0)
        far(3)
        far(1)

    def event6():
        far(2)

    lane = lax.broadcasted_iota(jnp.int32, (1, 128), 1)
    low = lane < 64
    ones = jnp.ones((128, 128), BF)
    row128 = lax.broadcasted_iota(jnp.int32, (128, 128), 0)
    col128 = lax.broadcasted_iota(jnp.int32, (128, 128), 1)
    head_ones = (
        (lax.broadcasted_iota(jnp.int32, (256, 256), 0) // 64)
        == (lax.broadcasted_iota(jnp.int32, (256, 256), 1) // 64)
    ).astype(F32).astype(BF)

    tpf = tp.astype(F32)
    s0 = sink[0]
    s1 = sink[1]
    m0 = jnp.maximum(s0, SHIFT)
    m1 = jnp.maximum(s1, SHIFT)
    for h in range(2):
        slope = jnp.exp2(jnp.full((128, 128), -(2.0 * tpf + (h + 1.0)) * 0.5, F32))
        m = (m0, m1)[h]
        for p in range(3):
            i = lax.broadcasted_iota(jnp.int32, (128, 128), 0)
            j = lax.broadcasted_iota(jnp.int32, (128, 128), 1)
            dist = jnp.abs(i - j - (128 * p - 128))
            val = (-slope * dist.astype(F32) - m) * LOG2E
            bias[p, 128 * h : 128 * h + 128, :] = jnp.where(dist <= 128, val, NEG)
        bias[3, 128 * h : 128 * h + 128, :] = jnp.full((128, 128), NEG, F32)

    hw = jnp.left_shift(jnp.int32(1), tp % 4)
    delta = (
        lax.broadcasted_iota(jnp.int32, (128, 256), 1)
        - 64
        - lax.broadcasted_iota(jnp.int32, (128, 256), 0)
    )
    band[...] = (
        ((delta + 1024) % 4 == 0) & (delta >= -4 * hw) & (delta <= 4 * hw - 4)
    ).astype(F32).astype(BF)

    for e in range(3):
        pos = lax.broadcasted_iota(jnp.int32, (512, 128), 0) // 4
        lo = pos - hw
        hi = pos + hw - 1
        if e == 1:
            lo = jnp.maximum(lo, 0)
        if e == 2:
            hi = jnp.minimum(hi, 127)
        inv[e] = 1.0 / (hi - lo + 1).astype(F32)

    if COMM:
        pl.semaphore_wait(barrier, 13)

    wcopies[0].wait()
    wcopies[1].wait()
    event0()

    def row_scale(x):
        sq = jnp.zeros((x.shape[0], 128), F32)
        for l in range(16):
            t = x[:, 128 * l : 128 * l + 128].astype(F32)
            sq = sq + t * t
        return lax.rsqrt(split_dot(sq, ones) * (1.0 / 2048) + EPS)

    xcopy(OWN).wait()
    r = row_scale(xb[tp].reshape(512, 2048))
    packed = [
        jnp.sum(jnp.where(row128 == col128, r[128 * g : 128 * g + 128], 0.0), axis=0, keepdims=True)
        for g in range(4)
    ]
    packed = jnp.concatenate(packed + [jnp.zeros((4, 128), F32)], axis=0)
    rsend[...] = packed
    rbuf[tp] = packed

    def rcopy(j, at):
        return remote(rsend, rbuf.at[at], rs_send.at[j], rs_recv.at[at], (sp, j))

    if COMM:
        for j in range(8):
            @pl.when(tp != j)
            def _():
                rcopy(j, tp).start()


    for cp in wcopies[2:]:
        cp.wait()
    for k in range(8):
        if k != OWN:
            xcopy(k).start()

    def prep(l, carry):
        rows = pl.ds(pl.multiple_of(l * 128, 128), 128)
        g = jnp.transpose(jnp.broadcast_to(gain[pl.ds(l, 1), :], (128, 128)))
        for t in (0, 1, 2, 4):
            cols = slice(128 * t, 128 * t + 128)
            wb[rows, cols] = (wb[rows, cols].astype(F32) * g).astype(BF)
        kv = jnp.transpose(kvt[:, rows].astype(F32))
        wb[rows, 384:512] = (kv * g).astype(BF)
        return carry

    lax.fori_loop(0, 16, prep, 0, unroll=2)

    qgain = jnp.concatenate([qg[...], qg[...]], axis=1) * (0.125 * LOG2E)
    kgain = jnp.concatenate([kg[...], kg[...]], axis=1)

    def halo(i, src, dst, dev):
        return remote(src, dst, hsend.at[i], hrecv.at[i], dev)

    def halo_left():
        return (
            halo(0, kvs.at[:, pl.ds(128, 128), :], kvs.at[:, pl.ds(9 * 128, 128), :], (sp - 1, tp)),
            halo(1, edge.at[pl.ds(0, 32)], poolbuf.at[pl.ds(64 + 4096, 32)], (sp - 1, tp)),
        )

    def halo_right():
        return (
            halo(2, kvs.at[:, pl.ds(8 * 128, 128), :], kvs.at[:, pl.ds(0, 128), :], (sp + 1, tp)),
            halo(3, edge.at[pl.ds(32, 32)], poolbuf.at[pl.ds(32, 32)], (sp + 1, tp)),
        )

    for cp in xedge:
        cp.wait()
    x = xe[...].reshape(64, 2048)
    edge[...] = (
        jnp.dot(x, wb[:, 0:128], preferred_element_type=F32) * row_scale(x)
    ).astype(BF)
    if COMM:
        @pl.when(sp > 0)
        def _():
            halo_left()[1].start()

        @pl.when(sp < NSP - 1)
        def _():
            halo_right()[1].start()

    event0_late()

    def multiply(k, lo, hi, at=None):
        p = (pa, pc)[k % 2]
        x = xb[order(k)].reshape(512, 2048)
        at = lo if at is None else at
        p[:, at : at + hi - lo] = jnp.dot(x, wb[:, lo:hi], preferred_element_type=F32)

    def slot(k):
        return 256 * ((k // 2) % 2)

    def ready(k):
        if COMM:
            blk = order(k)

            @pl.when(blk != tp)
            def _():
                rcopy(blk, blk).wait_recv()

    def scales(k):
        blk = order(k)
        return jnp.concatenate(
            [
                jnp.transpose(jnp.broadcast_to(rbuf[blk, g : g + 1, :], (128, 128)))
                for g in range(4)
            ],
            axis=0,
        )

    def finish_gates(k):
        blk = order(k)
        p = (pa, pc)[k % 2]
        at = slot(k)
        r = scales(k)
        rcol[k] = r
        rows = pl.ds(pl.multiple_of(blk * 512, 512), 512)
        prows = pl.ds(pl.multiple_of(blk * 512 + 64, 64), 512)
        poolbuf[prows, :] = (p[:, at : at + 128] * r).astype(BF)
        gate[rows, :] = (p[:, at + 128 : at + 256] * r).astype(BF)

    def finish_heads(k, r):
        blk = order(k)
        p = (pa, pc)[k % 2]
        rows = pl.ds(pl.multiple_of(blk * 512, 512), 512)
        agate[rows, :] = (p[:, 512:640] * r).astype(BF)
        q = (p[:, 256:384] * r).astype(BF).astype(F32)
        kv = (p[:, 384:512] * r).astype(BF).astype(F32)
        squares = jnp.concatenate([(q * q).astype(BF), (kv * kv).astype(BF)], axis=1)
        means = jnp.dot(squares, head_ones, preferred_element_type=F32) * (1.0 / 64)
        rq = lax.rsqrt(means[:, 0:128] + EPS)
        rk = lax.rsqrt(means[:, 128:256] + EPS)
        tmp[0] = q * rq * qgain
        tmp[1] = jnp.where(low, kv * rk * kgain, kv)
        for s in range(4):
            q = tmp[0, pl.ds(s, 128, stride=4), :]
            qs[blk, s, 0:128, :] = jnp.where(low, q, 0.0).astype(BF)
            qs[blk, s, 128:256, :] = jnp.where(low, pltpu.roll(q, 64, 1), 0.0).astype(BF)
            kvs[s, pl.ds(pl.multiple_of((blk + 1) * 128, 128), 128), :] = tmp[
                1, pl.ds(s, 128, stride=4), :
            ].astype(BF)

    def edges(k):
        if COMM:
            blk = order(k)

            @pl.when((blk == 0) & (sp > 0))
            def _():
                halo_left()[0].start()

            @pl.when((blk == 7) & (sp < NSP - 1))
            def _():
                halo_right()[0].start()

    def ahead(part):
        return (chip + 1 + 2 * ((c + part) % 2)) % 4

    def behind(part):
        return ((chip + 3 + 2 * ((c + part) % 2)) % 4) * 2 + c

    def direct(part, blk):
        return remote(
            ysend.at[part, blk], yr.at[part, tp], asend.at[part, blk], arecv.at[part, tp], (sp, blk)
        )

    def first_hop(part, blk):
        return remote(
            ysend.at[part, blk], relay.at[part, blk % 2], asend.at[part, blk], lrecv.at[part, blk % 2],
            (sp, ahead(part) * 2 + c),
        )

    def second_hop(part, e):
        return remote(
            relay.at[part, e], yr.at[part, behind(part)], lsend.at[part, e], arecv.at[part, behind(part)],
            (sp, ahead(part) * 2 + e),
        )

    def away(blk):
        return (blk // 2 - chip + 4) % 4

    def emit(part, blk):
        if COMM:
            @pl.when((blk != tp) & (away(blk) != 2))
            def _():
                direct(part, blk).start()

            @pl.when(away(blk) == 2)
            def _():
                first_hop(part, blk).start()

    def pass_on(part, e):
        if COMM:
            first_hop(part, e).wait_recv()
            second_hop(part, e).start()

    def pool_wait(blk):
        if COMM:
            @pl.when((blk == 0) & (sp > 0))
            def _():
                halo_right()[1].wait_recv()

            @pl.when((blk == 7) & (sp < NSP - 1))
            def _():
                halo_left()[1].wait_recv()

    def pool(blk):
        start = pl.multiple_of(blk * 512, 512)
        sums = jnp.concatenate(
            [
                jnp.dot(band[...], poolbuf[pl.ds(start + 128 * g, 256), :], preferred_element_type=F32)
                for g in range(4)
            ],
            axis=0,
        )
        scale = inv[sp0 * (1 - (blk + 7) // 8) + 2 * sp15 * ((blk + 1) // 8)]
        own = poolbuf[pl.ds(start + 64, 512), :].astype(F32)
        pooled = (sums * scale - own).astype(BF)
        mixed = jnp.dot(pooled, mix[0], preferred_element_type=F32)
        g = gate[pl.ds(start, 512), :].astype(F32)
        ysend[0, blk] = (mixed * silu(g)).astype(BF)

    def att_wait(blk):
        if COMM:
            @pl.when((blk == 0) & (sp > 0))
            def _():
                halo_right()[0].wait_recv()

            @pl.when((blk == 7) & (sp < NSP - 1))
            def _():
                halo_left()[0].wait_recv()

    def attend(blk):
        left = 3 * sp0 * (1 - (blk + 7) // 8)
        right = 2 + sp15 * ((blk + 1) // 8)
        for s in range(4):
            q = qs[blk, s]
            kv = kvs[s, pl.ds(pl.multiple_of(blk * 128, 128), 384), :]
            scores = lax.dot_general(q, kv, (((1,), (1,)), ((), ())), preferred_element_type=F32)
            w = jnp.concatenate(
                [
                    jnp.exp2(scores[:, 128 * p : 128 * p + 128] + bias[at]).astype(BF)
                    for p, at in ((0, left), (1, 1), (2, right))
                ],
                axis=1,
            )
            rhs = jnp.concatenate([kv, jnp.ones((384, 128), BF)], axis=1)
            o = jnp.dot(w, rhs, preferred_element_type=F32)
            t0 = o[0:128, 128:256] + jnp.exp(jnp.full((1, 128), s0 - m0, F32))
            t1 = o[128:256, 128:256] + jnp.exp(jnp.full((1, 128), s1 - m1, F32))
            over = jnp.where(low, pltpu.roll(o[0:128, 0:128], 64, 1), o[128:256, 0:128])
            att[pl.ds(s, 128, stride=4), :] = over / jnp.where(low, t0, t1)
            totals = jnp.log(jnp.transpose(jnp.where(lane == 0, t0, t1))[0:2, :])
            top = jnp.where(lax.broadcasted_iota(jnp.int32, (2, 128), 0) == 0, m0, m1)
            lse[s, :, pl.ds(pl.multiple_of(blk * 128, 128), 128)] = top + totals
        g = agate[pl.ds(pl.multiple_of(blk * 512, 512), 512), :].astype(F32)
        ysend[1, blk] = (att[...] * silu(g)).astype(BF)

    def gate_step(j):
        done = (2 * j - 2, 2 * j - 1) if j else ()
        pools = {2: (1, 2), 3: (3, 4), 4: (5, 6)}.get(j, ())
        for k in (2 * j, 2 * j + 1):
            if k < 8 and k != OWN:
                xcopy(k).wait()
        for k in done:
            ready(k)
        for k in pools:
            pool_wait(order(k))
        for i in range(2):
            if j < 4:
                multiply(2 * j + i, 0, 256, slot(2 * j + i))
            if done:
                finish_gates(done[i])
        for k in pools:
            pool(order(k))
        for k in pools:
            emit(0, order(k))

    def head_step(k):
        late = (7, 0)[k] if k < 2 else None
        if late is not None:
            pool_wait(order(late))
        if k in EARLY:
            att_wait(order(EARLY[k]))
        if k < 8:
            multiply(k, 256, 512)
        if k in EARLY:
            attend(order(EARLY[k]))
        if late is not None:
            pool(order(late))
        if k < 8:
            multiply(k, 512, 640)
        if k > 0:
            finish_heads(k - 1, rcol[k - 1])
            edges(k - 1)
        if late is not None:
            emit(0, order(late))
        if k in EARLY:
            emit(1, order(EARLY[k]))

    for j in range(5):
        gate_step(j)
        if j == 2:
            event1()
    for k in range(9):
        head_step(k)
        if k == 0:
            event2()
            pass_on(0, c)
        if k == 1:
            pass_on(0, 1 - c)
        if k == 4:
            event3()
        if k == 5:
            event4()
        if k == 7:
            event5()
        if k == 8:
            pass_on(1, c)

    def att_step(k, carry):
        blk = order((7 + k + (k // 2) * 4) % 8)
        att_wait(blk)
        attend(blk)
        emit(1, blk)
        if COMM:
            for at, event in ((0, event6), (2, functools.partial(pass_on, 1, 1 - c))):
                pl.when(k == at)(event)
        return carry

    lax.fori_loop(0, 4, att_step, 0)

    def arrive(part, j):
        if COMM:
            @pl.when(tp != j)
            def _():
                remote(
                    ysend.at[part, j], yr.at[part, j], asend.at[part, j], arecv.at[part, j], (sp, j)
                ).wait_recv()

    if COMM:
        for da in range(4):
            for db in range(4):
                if da or db:
                    ref = wg.at[1 - c, ((b_ + da) % 4) * sb + ((a + db) % 4) * sa]
                    remote(
                        ref, ref, dsend.at[da * 4 + db], drecv.at[da * 4 + db], (sp, tp + 1 - 2 * c)
                    ).wait_recv()

    for part in range(2):
        yr[part, tp] = ysend[part, tp]

    for j in range(8):
        arrive(0, j)

    def out_pool_step(n, carry):
        cols = pl.ds(pl.multiple_of(n * 512, 512), 512)
        acts = jnp.concatenate([yr[0, j] for j in range(8)], axis=1)
        acc[:, cols] = jnp.dot(
            acts, wg[0, :, :, cols].reshape(1024, 512), preferred_element_type=F32
        )
        return carry

    lax.fori_loop(0, 4, out_pool_step, 0)

    def attn_part(cols, d):
        src = [(chip + e) % 4 for e in d]
        acts = jnp.concatenate([yr[1, 2 * e + h] for e in src for h in range(2)], axis=1)
        rows = jnp.concatenate([wg[1, pl.ds(4 * e, 4), :, cols].reshape(256, 512) for e in src], axis=0)
        return acc[:, cols] + jnp.dot(acts, rows, preferred_element_type=F32)

    def out_near_step(n, carry):
        cols = pl.ds(pl.multiple_of(n * 512, 512), 512)
        acc[:, cols] = attn_part(cols, NEAR)
        return carry

    def out_attn_step(n, carry):
        cols = pl.ds(pl.multiple_of(n * 512, 512), 512)
        out[:, :, cols] = attn_part(cols, FAR).astype(BF).reshape(128, 4, 512)
        return carry

    for d in NEAR:
        for h in range(2):
            arrive(1, 2 * ((chip + d) % 4) + h)
    lax.fori_loop(0, 4, out_near_step, 0)
    for d in FAR:
        for h in range(2):
            arrive(1, 2 * ((chip + d) % 4) + h)
    lax.fori_loop(0, 4, out_attn_step, 0)

    if COMM:
        for part in range(2):
            for j in range(8):
                @pl.when(tp != j)
                def _():
                    direct(part, j).wait_send()
        for j in range(8):
            @pl.when(tp != j)
            def _():
                rcopy(j, tp).wait_send()
        for part in range(2):
            for e in range(2):
                second_hop(part, e).wait_send()
        for item in sends:
            gcopy(*item).wait_send()
        for da in range(4):
            for db in range(4):
                if da or db:
                    across(da, db).wait_send()

        @pl.when(sp > 0)
        def _():
            for cp in halo_left():
                cp.wait_send()

        @pl.when(sp < NSP - 1)
        def _():
            for cp in halo_right():
                cp.wait_send()


def layer(
    inputs, norm_gain, pool_proj, pool_gate_proj, pool_mix, query_proj, key_proj, value_proj,
    attn_gate_proj, query_gain, key_gain, sink_logit, out_pool, out_attn,
):
    hbm = pl.BlockSpec(memory_space=pl.ANY)
    vmem = pl.BlockSpec(memory_space=pltpu.VMEM)
    smem = pl.BlockSpec(memory_space=pltpu.SMEM)
    dma = pltpu.SemaphoreType.DMA
    mixed, log_sums = pl.pallas_call(
        kernel,
        out_shape=(
            pltpu.VMEM((128, 4, 2048), BF),
            pltpu.VMEM((4, 2, 1024), F32),
        ),
        in_specs=[hbm, vmem, hbm, hbm, hbm, hbm, hbm, hbm, vmem, vmem, vmem, smem, hbm, hbm],
        out_specs=(vmem, vmem),
        scratch_shapes=[
            pltpu.VMEM((8, 128, 4, 2048), BF),
            pltpu.VMEM((16, 4, 2048), BF),
            pltpu.VMEM((64, 128), BF),
            pltpu.VMEM((8, 512, 128), F32),
            pltpu.VMEM((2048, 640), BF),
            pltpu.VMEM((128, 2048), BF),
            pltpu.VMEM((512, 640), F32),
            pltpu.VMEM((512, 640), F32),
            pltpu.VMEM((2, 512, 128), F32),
            pltpu.VMEM((3, 512, 128), F32),
            pltpu.VMEM((8, 128), F32),
            pltpu.VMEM((8, 8, 128), F32),
            pltpu.VMEM((8, 4, 256, 128), BF),
            pltpu.VMEM((4, 1280, 128), BF),
            pltpu.VMEM((4096 + 128, 128), BF),
            pltpu.VMEM((4096, 128), BF),
            pltpu.VMEM((4096, 128), BF),
            pltpu.VMEM((4, 256, 128), F32),
            pltpu.VMEM((128, 256), BF),
            pltpu.VMEM((2, 8, 512, 128), BF),
            pltpu.VMEM((2, 8, 512, 128), BF),
            pltpu.VMEM((2, 16, 64, 2048), BF),
            pltpu.VMEM((512, 2048), F32),
            pltpu.VMEM((512, 128), F32),
            pltpu.VMEM((2, 2, 512, 128), BF),
            dma((10,)), dma((8,)), dma((8,)), dma((8,)), dma((2, 2)), dma((2, 2)),
            dma((2, 8)), dma((2, 8)),
            dma((4,)), dma((4,)),
            dma((24,)), dma((16, 2)),
            dma((16,)), dma((16,)),
        ],
        compiler_params=pltpu.CompilerParams(
            vmem_limit_bytes=60 * 1024 * 1024,
            **(dict(collective_id=0, has_side_effects=True) if COMM else {}),
        ),
        name="mixer_layer",
    )(
        inputs, norm_gain.reshape(16, 128), pool_proj, pool_gate_proj, query_proj, key_proj.T,
        value_proj.T, attn_gate_proj, pool_mix, query_gain.reshape(1, 64), key_gain.reshape(1, 64),
        sink_logit, out_pool, out_attn,
    )
    return mixed, jnp.transpose(log_sums, (2, 0, 1))


def solution(mesh):
    placed = (
        P("sp", None, None), P(), P(None, "tp"), P(None, "tp"), P("tp", None, None), P(None, "tp"),
        P(None, "tp"), P(None, "tp"), P(None, "tp"), P(), P(), P("tp"), P("sp", None), P("sp", None),
    )
    return jax.shard_map(
        layer,
        mesh=mesh,
        in_specs=placed,
        out_specs=(P(("sp", "tp"), None, None), P("sp", None, "tp")),
        check_vma=False,
    )
```

```python
import functools

import jax
import jax.numpy as jnp
from jax import lax
from jax.experimental import pallas as pl
from jax.experimental.pallas import tpu as pltpu
from jax.sharding import PartitionSpec as P

HEADS = 16
EPS = 1e-06
NEG = -1e30
SHIFT = 29.5
LOG2E = 1.4426950408889634
BF = jnp.bfloat16
F32 = jnp.float32
SEQ_LEN = 16384
NSP = 16
COMM = True
NEAR = (0, 2)
EARLY = {5: 1, 6: 3, 7: 2, 8: 4}
OWN = 5
FAR = (1, 3)


def split_dot(values, ones):
    hi = values.astype(BF)
    lo = (values - hi.astype(F32)).astype(BF)
    return jnp.dot(hi, ones, preferred_element_type=F32) + jnp.dot(lo, ones, preferred_element_type=F32)


def silu(v):
    return v / (1.0 + jnp.exp(-v))


def kernel(
    x_hbm, gain, pw, gw, qw, kw, vw, aw, mix, qg, kg, sink, outp, outa,
    out, lse,
    xb, xe, edge, rcol, wb, kvt, pa, pc, tmp, inv, rsend, rbuf, qs, kvs, poolbuf, gate, agate, bias, band, ysend, yr, wg, acc, att, relay,
    xsem, wsem, rs_send, rs_recv, lsend, lrecv, asend, arecv, hsend, hrecv, gsend, grecv, dsend, drecv,
):
    if COMM:
        sp = lax.axis_index("sp")
        tp = lax.axis_index("tp")
    else:
        sp = jnp.int32(0)
        tp = jnp.int32(0)
    chip = tp // 2
    c = tp % 2
    y = sp % 4
    z = sp // 4
    a = y * (1 - c) + z * c
    b_ = z * (1 - c) + y * c
    sa = 1 + 3 * c
    sb = 4 - 3 * c

    def order(k):
        return (2 * chip + 1 - c + (k + 2) - 2 * c * (k + 2) + 16) % 8

    def xcopy(k):
        return pltpu.make_async_copy(
            x_hbm.at[pl.ds(order(k) * 128, 128)], xb.at[order(k)], xsem.at[k]
        )

    xedge = (
        pltpu.make_async_copy(x_hbm.at[pl.ds(0, 8)], xe.at[pl.ds(0, 8)], xsem.at[8]),
        pltpu.make_async_copy(x_hbm.at[pl.ds(1016, 8)], xe.at[pl.ds(8, 8)], xsem.at[9]),
    )

    wcopies = [
        pltpu.make_async_copy(outp, wg.at[0, sp], wsem.at[0]),
        pltpu.make_async_copy(outa, wg.at[1, sp], wsem.at[1]),
        pltpu.make_async_copy(pw, wb.at[:, pl.ds(0, 128)], wsem.at[2]),
        pltpu.make_async_copy(gw, wb.at[:, pl.ds(128, 128)], wsem.at[3]),
        pltpu.make_async_copy(qw, wb.at[:, pl.ds(256, 128)], wsem.at[4]),
        pltpu.make_async_copy(kw, kvt.at[pl.ds(0, 64)], wsem.at[5]),
        pltpu.make_async_copy(vw, kvt.at[pl.ds(64, 64)], wsem.at[6]),
        pltpu.make_async_copy(aw, wb.at[:, pl.ds(512, 128)], wsem.at[7]),
    ]
    for cp in wcopies[:2]:
        cp.start()
    xcopy(OWN).start()
    for cp in wcopies[2:]:
        cp.start()
    for cp in xedge:
        cp.start()

    zeros = jnp.zeros((64, 128), BF)
    poolbuf[0:64, :] = zeros
    poolbuf[64 + 4096 : 128 + 4096, :] = zeros
    for s in range(4):
        kvs[s, 0:128, :] = jnp.zeros((128, 128), BF)
        kvs[s, 9 * 128 : 10 * 128, :] = jnp.zeros((128, 128), BF)

    def remote(src, dst, ss, rs, dev):
        return pltpu.make_async_remote_copy(
            src_ref=src, dst_ref=dst, send_sem=ss, recv_sem=rs,
            device_id=dev, device_id_type=pl.DeviceIdType.MESH,
        )

    if COMM:
        barrier = pltpu.get_barrier_semaphore()

        def greet(dev):
            pl.semaphore_signal(barrier, inc=1, device_id=dev, device_id_type=pl.DeviceIdType.MESH)

        for j in range(1, 8):
            greet((sp, (tp + j) % 8))
        greet((z * 4 + (y + 1) % 4, tp))
        greet((z * 4 + (y + 3) % 4, tp))
        greet((((z + 1) % 4) * 4 + y, tp))
        greet((((z + 3) % 4) * 4 + y, tp))

        greet(((sp + 1) % NSP, tp))
        greet(((sp + NSP - 1) % NSP, tp))

    sp0 = 1 - (sp + 15) // 16
    sp15 = (sp + 1) // 16

    def slice_at(da, db):
        return ((a + da) % 4) * sa + ((b_ + db) % 4) * sb

    def piece(da, db, half):
        if half is None:
            return wg.at[c, slice_at(da, db)]
        return wg.at[c, slice_at(da, db), pl.ds(32 * half, 32)]

    sends = []

    def gcopy(da, db, half, ma, mb, n):
        return remote(
            piece(da, db, half), piece(da, db, half), gsend.at[n],
            grecv.at[((da - ma) % 4) * 4 + (db - mb) % 4, half or 0],
            (slice_at(ma, mb), tp),
        )

    def send(da, db, half, ma, mb):
        if COMM:
            n = len(sends)
            sends.append((da, db, half, ma, mb, n))
            gcopy(da, db, half, ma, mb, n).start()

    def got(da, db, half=None):
        if COMM:
            ref = piece(da, db, half)
            remote(
                ref, ref, gsend.at[0], grecv.at[da * 4 + db, half or 0], (sp, tp + 1 - 2 * c)
            ).wait_recv()

    def across(da, db):
        ref = piece(da, db, None)
        return remote(
            ref, ref, dsend.at[da * 4 + db], drecv.at[da * 4 + db], (sp, tp + 1 - 2 * c)
        )

    def share(da, db):
        if COMM:
            across(da, db).start()

    def event0():
        send(0, 0, None, 1, 0)
        send(0, 0, None, -1, 0)

    def event0_late():
        send(0, 0, None, 0, 1)
        send(0, 0, None, 0, -1)

    def through(da):
        got(da, 3)
        send(da, 3, 0, 0, 1)
        share(da, 3)
        got(da, 1)
        send(da, 1, 1, 0, -1)
        share(da, 1)

    def far(da):
        got(da, 2, 0)
        got(da, 2, 1)
        share(da, 2)

    def event1():
        got(3, 0)
        send(3, 0, 0, 1, 0)
        got(1, 0)
        send(1, 0, 1, -1, 0)
        through(0)
        for da in (3, 1):
            send(da, 0, None, 0, 1)
            send(da, 0, None, 0, -1)
            share(da, 0)

    def event2():
        got(2, 0, 0)
        got(2, 0, 1)
        send(2, 0, None, 0, 1)
        send(2, 0, None, 0, -1)
        share(2, 0)

    def event3():
        through(3)
        through(1)

    def event4():
        through(2)

    def event5():
        far(0)
        far(3)
        far(1)

    def event6():
        far(2)

    lane = lax.broadcasted_iota(jnp.int32, (1, 128), 1)
    low = lane < 64
    ones = jnp.ones((128, 128), BF)
    row128 = lax.broadcasted_iota(jnp.int32, (128, 128), 0)
    col128 = lax.broadcasted_iota(jnp.int32, (128, 128), 1)
    head_ones = (
        (lax.broadcasted_iota(jnp.int32, (256, 256), 0) // 64)
        == (lax.broadcasted_iota(jnp.int32, (256, 256), 1) // 64)
    ).astype(F32).astype(BF)

    tpf = tp.astype(F32)
    s0 = sink[0]
    s1 = sink[1]
    m0 = jnp.maximum(s0, SHIFT)
    m1 = jnp.maximum(s1, SHIFT)
    for h in range(2):
        slope = jnp.exp2(jnp.full((128, 128), -(2.0 * tpf + (h + 1.0)) * 0.5, F32))
        m = (m0, m1)[h]
        for p in range(3):
            i = lax.broadcasted_iota(jnp.int32, (128, 128), 0)
            j = lax.broadcasted_iota(jnp.int32, (128, 128), 1)
            dist = jnp.abs(i - j - (128 * p - 128))
            val = (-slope * dist.astype(F32) - m) * LOG2E
            bias[p, 128 * h : 128 * h + 128, :] = jnp.where(dist <= 128, val, NEG)
        bias[3, 128 * h : 128 * h + 128, :] = jnp.full((128, 128), NEG, F32)

    hw = jnp.left_shift(jnp.int32(1), tp % 4)
    delta = (
        lax.broadcasted_iota(jnp.int32, (128, 256), 1)
        - 64
        - lax.broadcasted_iota(jnp.int32, (128, 256), 0)
    )
    band[...] = (
        ((delta + 1024) % 4 == 0) & (delta >= -4 * hw) & (delta <= 4 * hw - 4)
    ).astype(F32).astype(BF)

    for e in range(3):
        pos = lax.broadcasted_iota(jnp.int32, (512, 128), 0) // 4
        lo = pos - hw
        hi = pos + hw - 1
        if e == 1:
            lo = jnp.maximum(lo, 0)
        if e == 2:
            hi = jnp.minimum(hi, 127)
        inv[e] = 1.0 / (hi - lo + 1).astype(F32)

    if COMM:
        pl.semaphore_wait(barrier, 13)

    wcopies[0].wait()
    wcopies[1].wait()
    event0()

    def row_scale(x):
        sq = jnp.zeros((x.shape[0], 128), F32)
        for l in range(16):
            t = x[:, 128 * l : 128 * l + 128].astype(F32)
            sq = sq + t * t
        return lax.rsqrt(split_dot(sq, ones) * (1.0 / 2048) + EPS)

    xcopy(OWN).wait()
    r = row_scale(xb[tp].reshape(512, 2048))
    packed = [
        jnp.sum(jnp.where(row128 == col128, r[128 * g : 128 * g + 128], 0.0), axis=0, keepdims=True)
        for g in range(4)
    ]
    packed = jnp.concatenate(packed + [jnp.zeros((4, 128), F32)], axis=0)
    rsend[...] = packed
    rbuf[tp] = packed

    def rcopy(j, at):
        return remote(rsend, rbuf.at[at], rs_send.at[j], rs_recv.at[at], (sp, j))

    if COMM:
        for j in range(8):
            @pl.when(tp != j)
            def _():
                rcopy(j, tp).start()


    for cp in wcopies[2:]:
        cp.wait()
    for k in range(8):
        if k != OWN:
            xcopy(k).start()

    def prep(l, carry):
        rows = pl.ds(pl.multiple_of(l * 128, 128), 128)
        g = jnp.transpose(jnp.broadcast_to(gain[pl.ds(l, 1), :], (128, 128)))
        for t in (0, 1, 2, 4):
            cols = slice(128 * t, 128 * t + 128)
            wb[rows, cols] = (wb[rows, cols].astype(F32) * g).astype(BF)
        kv = jnp.transpose(kvt[:, rows].astype(F32))
        wb[rows, 384:512] = (kv * g).astype(BF)
        return carry

    lax.fori_loop(0, 16, prep, 0, unroll=2)

    qgain = jnp.concatenate([qg[...], qg[...]], axis=1) * (0.125 * LOG2E)
    kgain = jnp.concatenate([kg[...], kg[...]], axis=1)

    def halo(i, src, dst, dev):
        return remote(src, dst, hsend.at[i], hrecv.at[i], dev)

    def halo_left():
        return (
            halo(0, kvs.at[:, pl.ds(128, 128), :], kvs.at[:, pl.ds(9 * 128, 128), :], (sp - 1, tp)),
            halo(1, edge.at[pl.ds(0, 32)], poolbuf.at[pl.ds(64 + 4096, 32)], (sp - 1, tp)),
        )

    def halo_right():
        return (
            halo(2, kvs.at[:, pl.ds(8 * 128, 128), :], kvs.at[:, pl.ds(0, 128), :], (sp + 1, tp)),
            halo(3, edge.at[pl.ds(32, 32)], poolbuf.at[pl.ds(32, 32)], (sp + 1, tp)),
        )

    for cp in xedge:
        cp.wait()
    x = xe[...].reshape(64, 2048)
    edge[...] = (
        jnp.dot(x, wb[:, 0:128], preferred_element_type=F32) * row_scale(x)
    ).astype(BF)
    if COMM:
        @pl.when(sp > 0)
        def _():
            halo_left()[1].start()

        @pl.when(sp < NSP - 1)
        def _():
            halo_right()[1].start()

    event0_late()

    def multiply(k, lo, hi, at=None):
        p = (pa, pc)[k % 2]
        x = xb[order(k)].reshape(512, 2048)
        at = lo if at is None else at
        p[:, at : at + hi - lo] = jnp.dot(x, wb[:, lo:hi], preferred_element_type=F32)

    def slot(k):
        return 256 * ((k // 2) % 2)

    def ready(k):
        if COMM:
            blk = order(k)

            @pl.when(blk != tp)
            def _():
                rcopy(blk, blk).wait_recv()

    def scales(k):
        blk = order(k)
        return jnp.concatenate(
            [
                jnp.transpose(jnp.broadcast_to(rbuf[blk, g : g + 1, :], (128, 128)))
                for g in range(4)
            ],
            axis=0,
        )

    def finish_gates(k):
        blk = order(k)
        p = (pa, pc)[k % 2]
        at = slot(k)
        r = scales(k)
        rcol[k] = r
        rows = pl.ds(pl.multiple_of(blk * 512, 512), 512)
        prows = pl.ds(pl.multiple_of(blk * 512 + 64, 64), 512)
        poolbuf[prows, :] = (p[:, at : at + 128] * r).astype(BF)
        gate[rows, :] = (p[:, at + 128 : at + 256] * r).astype(BF)

    def finish_heads(k, r):
        blk = order(k)
        p = (pa, pc)[k % 2]
        rows = pl.ds(pl.multiple_of(blk * 512, 512), 512)
        agate[rows, :] = (p[:, 512:640] * r).astype(BF)
        q = (p[:, 256:384] * r).astype(BF).astype(F32)
        kv = (p[:, 384:512] * r).astype(BF).astype(F32)
        squares = jnp.concatenate([(q * q).astype(BF), (kv * kv).astype(BF)], axis=1)
        means = jnp.dot(squares, head_ones, preferred_element_type=F32) * (1.0 / 64)
        rq = lax.rsqrt(means[:, 0:128] + EPS)
        rk = lax.rsqrt(means[:, 128:256] + EPS)
        tmp[0] = q * rq * qgain
        tmp[1] = jnp.where(low, kv * rk * kgain, kv)
        for s in range(4):
            q = tmp[0, pl.ds(s, 128, stride=4), :]
            qs[blk, s, 0:128, :] = jnp.where(low, q, 0.0).astype(BF)
            qs[blk, s, 128:256, :] = jnp.where(low, pltpu.roll(q, 64, 1), 0.0).astype(BF)
            kvs[s, pl.ds(pl.multiple_of((blk + 1) * 128, 128), 128), :] = tmp[
                1, pl.ds(s, 128, stride=4), :
            ].astype(BF)

    def edges(k):
        if COMM:
            blk = order(k)

            @pl.when((blk == 0) & (sp > 0))
            def _():
                halo_left()[0].start()

            @pl.when((blk == 7) & (sp < NSP - 1))
            def _():
                halo_right()[0].start()

    def ahead(part):
        return (chip + 1 + 2 * ((c + part) % 2)) % 4

    def behind(part):
        return ((chip + 3 + 2 * ((c + part) % 2)) % 4) * 2 + c

    def direct(part, blk):
        return remote(
            ysend.at[part, blk], yr.at[part, tp], asend.at[part, blk], arecv.at[part, tp], (sp, blk)
        )

    def first_hop(part, blk):
        return remote(
            ysend.at[part, blk], relay.at[part, blk % 2], asend.at[part, blk], lrecv.at[part, blk % 2],
            (sp, ahead(part) * 2 + c),
        )

    def second_hop(part, e):
        return remote(
            relay.at[part, e], yr.at[part, behind(part)], lsend.at[part, e], arecv.at[part, behind(part)],
            (sp, ahead(part) * 2 + e),
        )

    def away(blk):
        return (blk // 2 - chip + 4) % 4

    def emit(part, blk):
        if COMM:
            @pl.when((blk != tp) & (away(blk) != 2))
            def _():
                direct(part, blk).start()

            @pl.when(away(blk) == 2)
            def _():
                first_hop(part, blk).start()

    def pass_on(part, e):
        if COMM:
            first_hop(part, e).wait_recv()
            second_hop(part, e).start()

    def pool_wait(blk):
        if COMM:
            @pl.when((blk == 0) & (sp > 0))
            def _():
                halo_right()[1].wait_recv()

            @pl.when((blk == 7) & (sp < NSP - 1))
            def _():
                halo_left()[1].wait_recv()

    def pool(blk):
        start = pl.multiple_of(blk * 512, 512)
        sums = jnp.concatenate(
            [
                jnp.dot(band[...], poolbuf[pl.ds(start + 128 * g, 256), :], preferred_element_type=F32)
                for g in range(4)
            ],
            axis=0,
        )
        scale = inv[sp0 * (1 - (blk + 7) // 8) + 2 * sp15 * ((blk + 1) // 8)]
        own = poolbuf[pl.ds(start + 64, 512), :].astype(F32)
        pooled = (sums * scale - own).astype(BF)
        mixed = jnp.dot(pooled, mix[0], preferred_element_type=F32)
        g = gate[pl.ds(start, 512), :].astype(F32)
        ysend[0, blk] = (mixed * silu(g)).astype(BF)

    def att_wait(blk):
        if COMM:
            @pl.when((blk == 0) & (sp > 0))
            def _():
                halo_right()[0].wait_recv()

            @pl.when((blk == 7) & (sp < NSP - 1))
            def _():
                halo_left()[0].wait_recv()

    def attend(blk):
        left = 3 * sp0 * (1 - (blk + 7) // 8)
        right = 2 + sp15 * ((blk + 1) // 8)
        for s in range(4):
            q = qs[blk, s]
            kv = kvs[s, pl.ds(pl.multiple_of(blk * 128, 128), 384), :]
            scores = lax.dot_general(q, kv, (((1,), (1,)), ((), ())), preferred_element_type=F32)
            w = jnp.concatenate(
                [
                    jnp.exp2(scores[:, 128 * p : 128 * p + 128] + bias[at]).astype(BF)
                    for p, at in ((0, left), (1, 1), (2, right))
                ],
                axis=1,
            )
            rhs = jnp.concatenate([kv, jnp.ones((384, 128), BF)], axis=1)
            o = jnp.dot(w, rhs, preferred_element_type=F32)
            t0 = o[0:128, 128:256] + jnp.exp(jnp.full((1, 128), s0 - m0, F32))
            t1 = o[128:256, 128:256] + jnp.exp(jnp.full((1, 128), s1 - m1, F32))
            over = jnp.where(low, pltpu.roll(o[0:128, 0:128], 64, 1), o[128:256, 0:128])
            att[pl.ds(s, 128, stride=4), :] = over / jnp.where(low, t0, t1)
            totals = jnp.log(jnp.transpose(jnp.where(lane == 0, t0, t1))[0:2, :])
            top = jnp.where(lax.broadcasted_iota(jnp.int32, (2, 128), 0) == 0, m0, m1)
            lse[s, :, pl.ds(pl.multiple_of(blk * 128, 128), 128)] = top + totals
        g = agate[pl.ds(pl.multiple_of(blk * 512, 512), 512), :].astype(F32)
        ysend[1, blk] = (att[...] * silu(g)).astype(BF)

    def gate_step(j):
        done = (2 * j - 2, 2 * j - 1) if j else ()
        pools = {2: (1, 2), 3: (3, 4), 4: (5, 6)}.get(j, ())
        for k in (2 * j, 2 * j + 1):
            if k < 8 and k != OWN:
                xcopy(k).wait()
        for k in done:
            ready(k)
        for k in pools:
            pool_wait(order(k))
        for i in range(2):
            if j < 4:
                multiply(2 * j + i, 0, 256, slot(2 * j + i))
            if done:
                finish_gates(done[i])
        for k in pools:
            pool(order(k))
        for k in pools:
            emit(0, order(k))

    def head_step(k):
        late = (7, 0)[k] if k < 2 else None
        if late is not None:
            pool_wait(order(late))
        if k in EARLY:
            att_wait(order(EARLY[k]))
        if k < 8:
            multiply(k, 256, 512)
        if k in EARLY:
            attend(order(EARLY[k]))
        if late is not None:
            pool(order(late))
        if k < 8:
            multiply(k, 512, 640)
        if k > 0:
            finish_heads(k - 1, rcol[k - 1])
            edges(k - 1)
        if late is not None:
            emit(0, order(late))
        if k in EARLY:
            emit(1, order(EARLY[k]))

    for j in range(5):
        gate_step(j)
        if j == 2:
            event1()
    for k in range(9):
        head_step(k)
        if k == 1:
            event2()
            pass_on(0, c)
        if k == 2:
            pass_on(0, 1 - c)
        if k == 4:
            event3()
        if k == 6:
            event4()
        if k == 7:
            event5()
        if k == 8:
            pass_on(1, c)

    def att_step(k, carry):
        blk = order((7 + k + (k // 2) * 4) % 8)
        att_wait(blk)
        attend(blk)
        emit(1, blk)
        if COMM:
            for at, event in ((0, event6), (2, functools.partial(pass_on, 1, 1 - c))):
                pl.when(k == at)(event)
        return carry

    lax.fori_loop(0, 4, att_step, 0)

    def arrive(part, j):
        if COMM:
            @pl.when(tp != j)
            def _():
                remote(
                    ysend.at[part, j], yr.at[part, j], asend.at[part, j], arecv.at[part, j], (sp, j)
                ).wait_recv()

    if COMM:
        for da in range(4):
            for db in range(4):
                if da or db:
                    ref = wg.at[1 - c, ((b_ + da) % 4) * sb + ((a + db) % 4) * sa]
                    remote(
                        ref, ref, dsend.at[da * 4 + db], drecv.at[da * 4 + db], (sp, tp + 1 - 2 * c)
                    ).wait_recv()

    for part in range(2):
        yr[part, tp] = ysend[part, tp]

    for j in range(8):
        arrive(0, j)

    def out_pool_step(n, carry):
        cols = pl.ds(pl.multiple_of(n * 512, 512), 512)
        acts = jnp.concatenate([yr[0, j] for j in range(8)], axis=1)
        acc[:, cols] = jnp.dot(
            acts, wg[0, :, :, cols].reshape(1024, 512), preferred_element_type=F32
        )
        return carry

    lax.fori_loop(0, 4, out_pool_step, 0, unroll=True)

    def attn_part(cols, d):
        src = [(chip + e) % 4 for e in d]
        acts = jnp.concatenate([yr[1, 2 * e + h] for e in src for h in range(2)], axis=1)
        rows = jnp.concatenate([wg[1, pl.ds(4 * e, 4), :, cols].reshape(256, 512) for e in src], axis=0)
        return acc[:, cols] + jnp.dot(acts, rows, preferred_element_type=F32)

    def out_near_step(n, carry):
        cols = pl.ds(pl.multiple_of(n * 512, 512), 512)
        acc[:, cols] = attn_part(cols, NEAR)
        return carry

    def out_attn_step(n, carry):
        cols = pl.ds(pl.multiple_of(n * 512, 512), 512)
        out[:, :, cols] = attn_part(cols, FAR).astype(BF).reshape(128, 4, 512)
        return carry

    for d in NEAR:
        for h in range(2):
            arrive(1, 2 * ((chip + d) % 4) + h)
    lax.fori_loop(0, 4, out_near_step, 0, unroll=True)
    for d in FAR:
        for h in range(2):
            arrive(1, 2 * ((chip + d) % 4) + h)
    lax.fori_loop(0, 4, out_attn_step, 0, unroll=True)

    if COMM:
        for part in range(2):
            for j in range(8):
                @pl.when(tp != j)
                def _():
                    direct(part, j).wait_send()
        for j in range(8):
            @pl.when(tp != j)
            def _():
                rcopy(j, tp).wait_send()
        for part in range(2):
            for e in range(2):
                second_hop(part, e).wait_send()
        for item in sends:
            gcopy(*item).wait_send()
        for da in range(4):
            for db in range(4):
                if da or db:
                    across(da, db).wait_send()

        @pl.when(sp > 0)
        def _():
            for cp in halo_left():
                cp.wait_send()

        @pl.when(sp < NSP - 1)
        def _():
            for cp in halo_right():
                cp.wait_send()


def layer(
    inputs, norm_gain, pool_proj, pool_gate_proj, pool_mix, query_proj, key_proj, value_proj,
    attn_gate_proj, query_gain, key_gain, sink_logit, out_pool, out_attn,
):
    hbm = pl.BlockSpec(memory_space=pl.ANY)
    vmem = pl.BlockSpec(memory_space=pltpu.VMEM)
    smem = pl.BlockSpec(memory_space=pltpu.SMEM)
    dma = pltpu.SemaphoreType.DMA
    mixed, log_sums = pl.pallas_call(
        kernel,
        out_shape=(
            pltpu.VMEM((128, 4, 2048), BF),
            pltpu.VMEM((4, 2, 1024), F32),
        ),
        in_specs=[hbm, vmem, hbm, hbm, hbm, hbm, hbm, hbm, vmem, vmem, vmem, smem, hbm, hbm],
        out_specs=(vmem, vmem),
        scratch_shapes=[
            pltpu.VMEM((8, 128, 4, 2048), BF),
            pltpu.VMEM((16, 4, 2048), BF),
            pltpu.VMEM((64, 128), BF),
            pltpu.VMEM((8, 512, 128), F32),
            pltpu.VMEM((2048, 640), BF),
            pltpu.VMEM((128, 2048), BF),
            pltpu.VMEM((512, 640), F32),
            pltpu.VMEM((512, 640), F32),
            pltpu.VMEM((2, 512, 128), F32),
            pltpu.VMEM((3, 512, 128), F32),
            pltpu.VMEM((8, 128), F32),
            pltpu.VMEM((8, 8, 128), F32),
            pltpu.VMEM((8, 4, 256, 128), BF),
            pltpu.VMEM((4, 1280, 128), BF),
            pltpu.VMEM((4096 + 128, 128), BF),
            pltpu.VMEM((4096, 128), BF),
            pltpu.VMEM((4096, 128), BF),
            pltpu.VMEM((4, 256, 128), F32),
            pltpu.VMEM((128, 256), BF),
            pltpu.VMEM((2, 8, 512, 128), BF),
            pltpu.VMEM((2, 8, 512, 128), BF),
            pltpu.VMEM((2, 16, 64, 2048), BF),
            pltpu.VMEM((512, 2048), F32),
            pltpu.VMEM((512, 128), F32),
            pltpu.VMEM((2, 2, 512, 128), BF),
            dma((10,)), dma((8,)), dma((8,)), dma((8,)), dma((2, 2)), dma((2, 2)),
            dma((2, 8)), dma((2, 8)),
            dma((4,)), dma((4,)),
            dma((24,)), dma((16, 2)),
            dma((16,)), dma((16,)),
        ],
        compiler_params=pltpu.CompilerParams(
            vmem_limit_bytes=60 * 1024 * 1024,
            **(dict(collective_id=0, has_side_effects=True) if COMM else {}),
        ),
        name="mixer_layer",
    )(
        inputs, norm_gain.reshape(16, 128), pool_proj, pool_gate_proj, query_proj, key_proj.T,
        value_proj.T, attn_gate_proj, pool_mix, query_gain.reshape(1, 64), key_gain.reshape(1, 64),
        sink_logit, out_pool, out_attn,
    )
    return mixed, jnp.transpose(log_sums, (2, 0, 1))


def solution(mesh):
    placed = (
        P("sp", None, None), P(), P(None, "tp"), P(None, "tp"), P("tp", None, None), P(None, "tp"),
        P(None, "tp"), P(None, "tp"), P(None, "tp"), P(), P(), P("tp"), P("sp", None), P("sp", None),
    )
    return jax.shard_map(
        layer,
        mesh=mesh,
        in_specs=placed,
        out_specs=(P(("sp", "tp"), None, None), P("sp", None, "tp")),
        check_vma=False,
    )
```
